256 devices in a mesh: ep: 64 (over z, y, core), tp: 4 (over x).
Axes of the slice: x: 4, y: 4, z: 8, core: 2. Of those that a mesh axis runs over, the one named last changes fastest.
Arguments:
- state_probe_logits: bfloat16 [65536, 1024], P('ep', 'tp'), may hold values from -6 to 6
- retention_logits: bfloat16 [65536, 1024], P('ep', 'tp'), may hold values from -12 to 12
- state_source_entries: bfloat16 [65536, 1024], P('ep', 'tp'), may hold values from -6 to 6
- state_result_switch_logits: bfloat16 [65536, 1024], P('ep', 'tp'), may hold values from -6 to 6
- retention_bound_margin: float32 [1024], P('tp'), may hold values from 0 to 0.07
- extra_fading_amount: float32 [65536, 8], P('ep', 'tp'), may hold values from -0.7 to 0
- state_result_scale: float32 [1024], P('tp'), may hold values from 0.1 to 1.9
- state_result_matrix: bfloat16 [1024, 2048], P(None, 'tp'), may hold values from -0.1875 to 0.1875
- second_slice_tokens: bfloat16 [32768, 2048], P('ep'), may hold values from -6 to 6
- specialist_assignment: int32 [32768, 2], P('ep'), may hold values from 0 to 63, all different within a row; in each aligned block of 128 rows (0 to 127, 128 to 255, ...) at most 8 rows name the same one
- selected_specialist_share: float32 [32768, 2], P('ep'), may hold values from 0.1 to 1
- leading_scale_vector: float32 [2048], replicated, may hold values from 0.1 to 1.9
- trailing_scale_vector: float32 [2048], replicated, may hold values from 0.1 to 1.9
- specialist_switch_matrix: bfloat16 [64, 2048, 2048], P('ep', None, 'tp'), may hold values from -0.3125 to 0.3125
- specialist_widen_matrix: bfloat16 [64, 2048, 2048], P('ep', None, 'tp'), may hold values from -0.3125 to 0.3125
- specialist_contract_matrix: bfloat16 [64, 2048, 2048], P('ep', 'tp'), may hold values from -0.125 to 0.125
Outputs:
- mixer_out: bfloat16 [65536, 2048], P('ep', 'tp')
- moe_out: bfloat16 [32768, 2048], P(('ep', 'tp'))
The draws below stay inside these ranges and needn't reach their ends.
Inputs may be any that keep to these rules, and one draw needn't show every extreme that they name: `specialist_assignment`: each row names 2 different experts. In each aligned block of 128 rows no expert is named by more than 8 rows, a bound that some block reaches.
All inputs are finite; a program needn't handle non-finite values.
Results may differ from the reference program's by a relative error of at most 0.012.
Values may be sent and summed in bfloat16 or wider, within the bound.
No kernel may reach another device: no remote copies, remote signals or barrier semaphores. Data moves between devices by JAX's collectives and lax.ppermute only.
A program may use at most 128 MiB of HBM per device.

```python
import math
import jax
import jax.numpy as jnp
import numpy as np
from jax import lax

D = 2048
HEAD = 128
STATE_GROUPS = 8
STATE_FEATURES = 1024
SPAN_STEPS = 64
FFE = 2048
EXPERTS = 64
TOP_K = 2
MIX_EP = 1024
TOK_DEV = 128
MIX_TOKENS = 65536
MOE_TOKENS = 32768
CAPQ = 8
N_TP = 4


def draw_retention_logits(key, part):
    noise_key, shift_key = jax.random.split(key)
    span_rows = max(MIX_EP // 4, 1)
    span_count = MIX_TOKENS // span_rows
    noise = jax.random.normal(noise_key, (MIX_TOKENS, STATE_FEATURES), jnp.float32)
    shifts = jax.random.uniform(shift_key, (span_count,), jnp.float32, -1.0, 1.5)
    return (noise + jnp.repeat(shifts, span_rows)[:, None]).astype(jnp.bfloat16)


def draw_retention_bound_margin(key, part):
    head_key, slow_key, fast_key = jax.random.split(key, 3)
    picked = jax.random.uniform(head_key, (STATE_GROUPS,), jnp.float32)
    slow_heads = picked < 0.5
    slow_channel = jnp.repeat(slow_heads, HEAD)
    lower = math.log(0.5 / MIX_TOKENS)
    upper = math.log(4.0 / MIX_TOKENS)
    slow_gap = jnp.exp(jax.random.uniform(slow_key, (STATE_FEATURES,), jnp.float32, lower, upper))
    fast_gap = jax.random.uniform(fast_key, (STATE_FEATURES,), jnp.float32, 0.03, 0.07)
    return jnp.where(slow_channel, slow_gap, fast_gap)


def draw_extra_fading_amount(key, part):
    where_key, depth_key = jax.random.split(key)
    struck = jax.random.uniform(where_key, (MIX_TOKENS, STATE_GROUPS), jnp.float32) < 6.0 / MIX_TOKENS
    depth = jnp.log(jax.random.uniform(depth_key, (MIX_TOKENS, STATE_GROUPS), jnp.float32, 0.5, 0.8))
    return jnp.where(struck, depth, jnp.zeros((), jnp.float32))


def block_levels(key, dims, pieces, smallest, largest):
    level = 1.0
    for position, shards_of in pieces:
        steps = jax.random.uniform(jax.random.fold_in(jax.random.fold_in(key, 6), position), (shards_of,), jnp.float32, smallest / len(pieces), largest / len(pieces))
        level = level * jnp.repeat(jnp.exp(steps), dims[position] // shards_of).reshape((-1,) + (1,) * (len(dims) - 1 - position))
    return level


def deal_out(key, own, number, rows, count, top, reach, lean):
    order = jax.random.permutation(key, count)
    packed, ordinary = shares(count, rows * top, reach, lean, True), shares(count, rows * top, reach, lean, False)
    places = jnp.arange(count)

    def named(tallies, rotation):
        used = int((tallies > 0).sum())
        fixed = max(1, used // 4)
        passed = fixed + (places - fixed + rotation * (used - fixed)) % max(1, count - fixed)
        return jnp.zeros((count,), jnp.int32).at[order[jnp.where(places < fixed, places, passed)]].set(jnp.asarray(tallies, jnp.int32))

    tallies = jnp.where(number % 4 == 0, named(packed, number // 4), named(ordinary, number - number // 4 - 1))
    mixed = jax.random.permutation(jax.random.fold_in(own, 3), count)
    giver, receiver = mixed[0:count // 2 * 2:2], mixed[1:count // 2 * 2:2]
    slack = jnp.minimum(tallies[giver] - 1, reach - tallies[receiver]) // 2
    slack = jnp.where((giver == order[0]) | (receiver == order[0]) | (tallies[receiver] == 0), 0, jnp.maximum(slack, 0))
    passed = jax.random.randint(jax.random.fold_in(own, 4), (count // 2,), 0, 1 << 20) % (slack + 1)
    tallies = tallies.at[giver].add(-passed).at[receiver].add(passed)
    labels = jnp.searchsorted(jnp.cumsum(tallies), jnp.arange(rows * top), side="right").astype(jnp.int32)
    grid = labels.reshape(top, rows).T
    grid = grid[jax.random.permutation(jax.random.fold_in(own, 1), rows)]
    rotation = jax.random.randint(jax.random.fold_in(own, 2), (rows, 1), 0, top)
    return jnp.take_along_axis(grid, (jnp.arange(top)[None, :] + rotation) % top, axis=1)


def shares(count, total, limit, lean, full):
    weights = [(1 << 20) // math.isqrt(standing ** lean) + 1 for standing in range(1, count + 1)]
    largest = limit if full else min(limit, max(-(-total // count), total * weights[0] // sum(weights)))
    least = 1 if total - largest >= count - 1 else 0
    counts, surplus = [largest] + [least] * (count - 1), total - largest - least * (count - 1)
    while surplus > 0:
        candidates = [i for i in range(1, count) if counts[i] < largest] or [i for i in range(1, count) if counts[i] < limit]
        mass, remaining = sum([weights[i] for i in candidates]), surplus
        for i in candidates:
            addition = min(limit - counts[i], max(1, remaining * weights[i] // mass), surplus)
            counts[i] = counts[i] + addition
            surplus = surplus - addition
    return np.array(counts)


def normal_values(stream_key, shape, scale, most, pieces=(), held_as=jnp.bfloat16):
    drawn = scale * jax.random.normal(stream_key, shape, jnp.float32)
    if pieces:
        drawn = drawn * block_levels(stream_key, shape, pieces, -0.22, 0.18)
    return jnp.clip(drawn, -most, most).astype(held_as)


def setup_inputs(seed: int = 0) -> dict:
    seeds = jax.random.split(jax.random.key(seed), 17)
    state_probe_logits = normal_values(seeds[0], (MIX_TOKENS, STATE_FEATURES), 1.0, 6.0, ((0, 64), (1, 4)))
    retention_logits = draw_retention_logits(jax.random.fold_in(seeds[16], 71), 0)
    state_source_entries = normal_values(seeds[2], (MIX_TOKENS, STATE_FEATURES), 1.0, 6.0, ((0, 64), (1, 4)))
    state_result_switch_logits = normal_values(seeds[3], (MIX_TOKENS, STATE_FEATURES), 1.0, 6.0, ((0, 64), (1, 4)))
    retention_bound_margin = draw_retention_bound_margin(jax.random.fold_in(seeds[16], 71), 0)
    extra_fading_amount = draw_extra_fading_amount(jax.random.fold_in(seeds[16], 71), 0)
    state_result_scale = jnp.clip(1.0 + 0.18 * jax.random.normal(seeds[6], (STATE_FEATURES,), jnp.float32), 0.1, 1.9)
    state_result_matrix = normal_values(seeds[7], (STATE_FEATURES, D), STATE_FEATURES ** -0.5, 0.1875, ((1, 4),))
    second_slice_tokens = normal_values(seeds[8], (MOE_TOKENS, D), 1.0, 6.0, ((0, 64),))
    specialist_assignment_keys = jax.random.split(jax.random.fold_in(seeds[9], 1), MOE_TOKENS // TOK_DEV)
    specialist_assignment_turns = jax.random.permutation(jax.random.fold_in(seeds[9], 3), MOE_TOKENS // TOK_DEV)
    specialist_assignment = jax.vmap(lambda own, number: deal_out(jax.random.fold_in(seeds[9], 2), own, number, TOK_DEV, EXPERTS, TOP_K, CAPQ, 1))(specialist_assignment_keys, specialist_assignment_turns).reshape((MOE_TOKENS, TOP_K))
    selected_specialist_share = jnp.clip(jnp.exp(math.log(1.0) - 2.3025851 * jax.random.uniform(seeds[10], (MOE_TOKENS, TOP_K), jnp.float32) ** block_levels(seeds[10], (MOE_TOKENS, TOP_K), ((0, 64),), -0.2, 0.2)), 0.1, 1.0)
    leading_scale_vector = jnp.clip(1.0 + 0.18 * jax.random.normal(seeds[11], (D,), jnp.float32), 0.1, 1.9)
    trailing_scale_vector = jnp.clip(1.0 + 0.18 * jax.random.normal(seeds[12], (D,), jnp.float32), 0.1, 1.9)
    specialist_switch_matrix = normal_values(seeds[13], (EXPERTS, D, FFE), (D // 6) ** -0.5, 0.3125, ((0, 64), (2, 4)))
    specialist_widen_matrix = normal_values(seeds[14], (EXPERTS, D, FFE), (D // 6) ** -0.5, 0.3125, ((0, 64), (2, 4)))
    specialist_contract_matrix = normal_values(seeds[15], (EXPERTS, FFE, D), FFE ** -0.5, 0.125, ((0, 64), (1, 4)))
    return dict(state_probe_logits=state_probe_logits, retention_logits=retention_logits, state_source_entries=state_source_entries, state_result_switch_logits=state_result_switch_logits, retention_bound_margin=retention_bound_margin, extra_fading_amount=extra_fading_amount, state_result_scale=state_result_scale, state_result_matrix=state_result_matrix, second_slice_tokens=second_slice_tokens, specialist_assignment=specialist_assignment, selected_specialist_share=selected_specialist_share, leading_scale_vector=leading_scale_vector, trailing_scale_vector=trailing_scale_vector, specialist_switch_matrix=specialist_switch_matrix, specialist_widen_matrix=specialist_widen_matrix, specialist_contract_matrix=specialist_contract_matrix)


NORM_EPS = 1e-06
SWISH_ALPHA = 1.702
CLAMP_LIMIT = 7.0
EXACT = lax.Precision.HIGHEST

def rms_scale(values, gain):
    return values * lax.rsqrt(lax.optimization_barrier(jnp.mean(values * values, axis=-1, keepdims=True)) + NORM_EPS) * gain

def clamped_unit(gate, upward):
    glued = jnp.minimum(gate, CLAMP_LIMIT)
    linear = jnp.clip(upward, -CLAMP_LIMIT, CLAMP_LIMIT)
    return glued * jax.nn.sigmoid(SWISH_ALPHA * glued) * (linear + 1.0)

def state_space_layer(state_probe_logits, retention_logits, state_source_entries, state_result_switch_logits, retention_bound_margin, extra_fading_amount, state_result_scale):
    total_rows = state_probe_logits.shape[0]
    span_tally = total_rows // SPAN_STEPS
    causal = jnp.tril(jnp.ones((SPAN_STEPS, SPAN_STEPS), jnp.float32))

    def per_head(values):
        return values.reshape(SPAN_STEPS, STATE_GROUPS, HEAD).transpose(1, 0, 2)

    def advance(state, operand_tensors):
        query_preact, forget_preact, value_preact, micro_batch_rows = operand_tensors
        query = per_head(jax.nn.silu(query_preact.astype(jnp.float32)) * HEAD ** (-0.5))
        input_key = per_head(retention_bound_margin * jax.nn.sigmoid(-forget_preact.astype(jnp.float32)))
        decay_logarithm = jnp.log1p(-input_key) + micro_batch_rows.T[:, :, None]
        values = per_head(value_preact.astype(jnp.float32))
        cumul = jnp.cumsum(decay_logarithm, axis=1)
        middle = cumul[:, SPAN_STEPS // 2 - 1:SPAN_STEPS // 2]
        last = cumul[:, SPAN_STEPS - 1:]
        scores = jnp.einsum('hid,hjd->hij', query * jnp.exp(cumul - middle), input_key * jnp.exp(middle - cumul), precision=EXACT) * causal
        inner = jnp.einsum('hij,hje->hie', scores, values, precision=EXACT)
        outer = jnp.einsum('hid,hde->hie', query * jnp.exp(cumul), state, precision=EXACT)
        update = jnp.einsum('hcd,hce->hde', input_key * jnp.exp(last - cumul), values, precision=EXACT)
        state = jnp.exp(last[:, 0])[:, :, None] * state + update
        return (state, inner + outer)
    operand_tensors = (state_probe_logits.reshape(span_tally, SPAN_STEPS, STATE_FEATURES), retention_logits.reshape(span_tally, SPAN_STEPS, STATE_FEATURES), state_source_entries.reshape(span_tally, SPAN_STEPS, STATE_FEATURES), extra_fading_amount.reshape(span_tally, SPAN_STEPS, STATE_GROUPS))
    final_state, raw_out = lax.scan(advance, jnp.zeros((STATE_GROUPS, HEAD, HEAD), jnp.float32), operand_tensors)
    normed = raw_out * lax.rsqrt(lax.optimization_barrier(jnp.mean(raw_out * raw_out, axis=-1, keepdims=True)) + NORM_EPS)
    normed = normed.transpose(0, 2, 1, 3).reshape(total_rows, STATE_FEATURES)
    return (normed * state_result_scale * jax.nn.silu(state_result_switch_logits.astype(jnp.float32))).astype(jnp.bfloat16)

def experts(second_slice_tokens, specialist_assignment, selected_specialist_share, leading_scale_vector, trailing_scale_vector, specialist_switch_matrix, specialist_widen_matrix, specialist_contract_matrix):
    token_count = second_slice_tokens.shape[0]
    span_tally = token_count // TOK_DEV
    normed = rms_scale(second_slice_tokens.astype(jnp.float32), leading_scale_vector).astype(jnp.bfloat16)
    per_block = TOK_DEV * TOP_K
    flat = specialist_assignment.reshape(span_tally, per_block)
    onehot = (flat[:, :, None] == jnp.arange(EXPERTS, dtype=jnp.int32)[None, None, :]).astype(jnp.int32)
    rank = lax.optimization_barrier(jnp.sum(onehot * (jnp.cumsum(onehot, axis=1) - 1), axis=2))
    slots = ((flat * span_tally + jnp.arange(span_tally, dtype=jnp.int32)[:, None]) * CAPQ + rank).reshape(-1)
    owner = jnp.arange(token_count * TOP_K, dtype=jnp.int32) // TOP_K
    per_expert = span_tally * CAPQ
    room = EXPERTS * per_expert
    source = jnp.zeros((room,), jnp.int32).at[slots].set(owner)
    filled = jnp.zeros((room,), jnp.int32).at[slots].set(1)
    width = FFE // N_TP

    def one_expert(operand_tensors):
        rows_source, rows_live, gate_w, up_w, down_w = operand_tensors
        chosen = jnp.where(rows_live[:, None] > 0, normed[rows_source], jnp.zeros((), jnp.bfloat16))
        gate = jnp.dot(chosen, gate_w, preferred_element_type=jnp.float32)
        upward = jnp.dot(chosen, up_w, preferred_element_type=jnp.float32)
        activated = clamped_unit(gate, upward).astype(jnp.bfloat16)
        parts = jnp.einsum('rjf,jfd->jrd', activated.reshape(per_expert, N_TP, width).astype(jnp.float32), down_w.reshape(N_TP, width, D).astype(jnp.float32))
        parts = lax.optimization_barrier(parts.astype(jnp.bfloat16))
        return lax.optimization_barrier(jnp.sum(parts.astype(jnp.float32), axis=0)).astype(jnp.bfloat16)
    outputs = lax.map(one_expert, (source.reshape(EXPERTS, per_expert), filled.reshape(EXPERTS, per_expert), specialist_switch_matrix, specialist_widen_matrix, specialist_contract_matrix))
    flat_out = outputs.reshape(room, D)
    token_slots = slots.reshape(token_count, TOP_K)
    combined = jnp.zeros((token_count, D), jnp.float32)
    for column in range(TOP_K):
        combined = combined + flat_out[token_slots[:, column]].astype(jnp.float32) * selected_specialist_share[:, column:column + 1]
    return rms_scale(combined, trailing_scale_vector).astype(jnp.bfloat16)

def reference(state_probe_logits, retention_logits, state_source_entries, state_result_switch_logits, retention_bound_margin, extra_fading_amount, state_result_scale, state_result_matrix, second_slice_tokens, specialist_assignment, selected_specialist_share, leading_scale_vector, trailing_scale_vector, specialist_switch_matrix, specialist_widen_matrix, specialist_contract_matrix):
    state_layer_result = state_space_layer(state_probe_logits, retention_logits, state_source_entries, state_result_switch_logits, retention_bound_margin, extra_fading_amount, state_result_scale)
    mixer_out = jnp.dot(state_layer_result, state_result_matrix, preferred_element_type=jnp.float32).astype(jnp.bfloat16)
    moe_out = experts(second_slice_tokens, specialist_assignment, selected_specialist_share, leading_scale_vector, trailing_scale_vector, specialist_switch_matrix, specialist_widen_matrix, specialist_contract_matrix)
    return (mixer_out, moe_out)
```

```python
import functools

import jax
import jax.numpy as jnp
from jax import lax
from jax.experimental import pallas as pl
from jax.experimental.pallas import tpu as pltpu
from jax.sharding import Mesh
from jax.sharding import PartitionSpec as P

HEAD = 128
SPAN = 128
TOK_DEV = 128
EP = ("ep_0", "ep_1", "ep_2")
EP_TP = ("ep_0", "ep_1", "ep_2", "tp")
GROUPS = 2


NORM_EPS = 1e-06
SWISH_ALPHA = 1.702
CLAMP_LIMIT = 7.0

F32 = jnp.float32
BF16 = jnp.bfloat16


def rms_scale(values, gain):
    return values * lax.rsqrt(jnp.mean(values * values, axis=-1, keepdims=True) + NORM_EPS) * gain


def clamped_unit(gate, upward):
    glued = jnp.minimum(gate, CLAMP_LIMIT)
    linear = jnp.clip(upward, -CLAMP_LIMIT, CLAMP_LIMIT)
    return glued * jax.nn.sigmoid(SWISH_ALPHA * glued) * (linear + 1.0)


def log_one_minus(x):
    total = jnp.full_like(x, 1.0 / 9.0)
    for k in range(8, 0, -1):
        total = total * x + 1.0 / k
    return -(x * total)


def split3(x):
    hi = x.astype(BF16)
    rest = x - hi.astype(F32)
    mid = rest.astype(BF16)
    low = (rest - mid.astype(F32)).astype(BF16)
    return hi, mid, low


def local_kernel(q_ref, r_ref, v_ref, m_ref, fade_ref, raw_ref, qdec_ref, st_ref):
    rows, width = q_ref.shape
    heads = width // HEAD
    steps = rows // SPAN
    row = lax.broadcasted_iota(jnp.int32, (SPAN, SPAN), 0)
    col = lax.broadcasted_iota(jnp.int32, (SPAN, SPAN), 1)
    lower = row >= col
    tri = lower.astype(F32).astype(BF16)
    margin = m_ref[...]

    def step(n, carry):
        base, states = carry
        at = pl.ds(pl.multiple_of(n * SPAN, SPAN), SPAN)
        q = q_ref[at, :].astype(F32)
        q = q / (1.0 + jnp.exp(-q)) * HEAD ** (-0.5)
        key = margin / (1.0 + jnp.exp(r_ref[at, :].astype(F32)))
        value = v_ref[at, :]
        fade = fade_ref[at, :]
        fade = jnp.concatenate(
            [jnp.broadcast_to(fade[:, h : h + 1], (SPAN, HEAD)) for h in range(heads)], axis=1
        )
        decay = log_one_minus(key) + fade
        cumul = sum(
            jnp.dot(tri, piece, preferred_element_type=F32) for piece in reversed(split3(decay))
        )
        middle = cumul[SPAN // 2 - 1 : SPAN // 2, :]
        last = cumul[SPAN - 1 : SPAN, :]
        grow = jnp.exp(cumul - middle)
        q_mid = (q * grow).astype(BF16)
        k_mid = (key * jnp.exp(middle - cumul)).astype(BF16)
        q_start = (q * jnp.exp(cumul)).astype(BF16)
        k_end = (key * jnp.exp(last - cumul)).astype(BF16)
        qdec_ref[at, :] = (q * jnp.exp(cumul + base)).astype(BF16)
        block_decay = jnp.exp(last)
        after = []
        for h in range(heads):
            c = slice(h * HEAD, (h + 1) * HEAD)
            scores = lax.dot_general(
                q_mid[:, c], k_mid[:, c], (((1,), (1,)), ((), ())), preferred_element_type=F32
            )
            scores = jnp.where(lower, scores, 0.0).astype(BF16)
            inner = jnp.dot(scores, value[:, c], preferred_element_type=F32)
            outer = jnp.dot(q_start[:, c], states[h].astype(BF16), preferred_element_type=F32)
            raw_ref[at, c] = inner + outer
            update = lax.dot_general(
                k_end[:, c], value[:, c], (((0,), (0,)), ((), ())), preferred_element_type=F32
            )
            wide = jnp.transpose(jnp.broadcast_to(block_decay[:, c], (HEAD, HEAD)))
            after.append(wide * states[h] + update)
        return base + last, tuple(after)

    base, states = lax.fori_loop(
        0,
        steps,
        step,
        (jnp.zeros((1, width), F32), tuple(jnp.zeros((HEAD, HEAD), F32) for _ in range(heads))),
    )
    total = jnp.exp(base)
    for h in range(heads):
        c = slice(h * HEAD, (h + 1) * HEAD)
        st_ref[c, :HEAD] = states[h]
        st_ref[c, HEAD:] = jnp.transpose(jnp.broadcast_to(total[:, c], (HEAD, HEAD)))


def prefix_kernel(x_ref, out_ref):
    state = jnp.zeros(out_ref.shape[1:], F32)
    for i in range(x_ref.shape[0]):
        out_ref[i] = state
        state = x_ref[i, :, HEAD:] * state + x_ref[i, :, :HEAD]


def output_kernel(raw_ref, qdec_ref, e_ref, gate_ref, scale_ref, out_ref):
    rows, width = raw_ref.shape
    tile = 256

    def step(n, carry):
        at = pl.ds(pl.multiple_of(n * tile, tile), tile)
        for h in range(width // HEAD):
            c = slice(h * HEAD, (h + 1) * HEAD)
            raw = raw_ref[at, c] + jnp.dot(
                qdec_ref[at, c], e_ref[c, :], preferred_element_type=F32
            )
            normed = raw * lax.rsqrt(jnp.mean(raw * raw, axis=-1, keepdims=True) + NORM_EPS)
            gate = gate_ref[at, c].astype(F32)
            out_ref[at, c] = (
                normed * scale_ref[:, c] * (gate / (1.0 + jnp.exp(-gate)))
            ).astype(BF16)
        return carry

    lax.fori_loop(0, rows // tile, step, 0)


def vmem_call(kernel, outs, flops, bytes_accessed, transcendentals, name):
    return pl.pallas_call(
        kernel,
        out_shape=outs,
        cost_estimate=pl.CostEstimate(
            flops=flops, bytes_accessed=bytes_accessed, transcendentals=transcendentals
        ),
        name=name,
    )


def local_pass(q, r, v, margin, fade):
    rows, width = q.shape
    return vmem_call(
        local_kernel,
        (
            jax.ShapeDtypeStruct((rows, width), F32),
            jax.ShapeDtypeStruct((rows, width), BF16),
            jax.ShapeDtypeStruct((width, 2 * HEAD), F32),
        ),
        4_000_000_000,
        6 << 20,
        rows * width * 6,
        "local_pass",
    )(q, r, v, margin.reshape(1, width), fade)


def prefix_pass(x):
    return vmem_call(
        prefix_kernel,
        jax.ShapeDtypeStruct((x.shape[0], x.shape[1], HEAD), F32),
        100_000_000,
        1 << 19,
        0,
        "prefix_pass",
    )(x)


def output_pass(raw, qdec, entering, gate, scale):
    rows, width = raw.shape
    return vmem_call(
        output_kernel,
        jax.ShapeDtypeStruct((rows, width), BF16),
        2_000_000_000,
        4 << 20,
        rows * width * 2,
        "output_pass",
    )(raw, qdec, entering, gate, scale.reshape(1, width))


def shift(x, by):
    n = lax.axis_size("tp")
    return lax.ppermute(x, "tp", [(i, (i + by) % n) for i in range(n)])


def ring_gather(own):
    half = own.shape[0] // 2
    left = shift(own, 1)
    right = shift(own, -1)
    far_top = shift(left[:half], 1)
    far_bottom = shift(right[half:], -1)
    return own, left, right, jnp.concatenate([far_top, far_bottom], axis=0)


def across(x):
    half = x.shape[0] // 2
    top = shift(shift(x[:half], 1), 1)
    bottom = shift(shift(x[half:], -1), -1)
    return jnp.concatenate([top, bottom], axis=0)


def widened(weight, dim):
    half = weight.shape[dim] // 2
    first = lax.slice_in_dim(weight, 0, half, axis=dim)
    second = lax.slice_in_dim(weight, half, 2 * half, axis=dim)
    return jnp.concatenate([weight, shift(first, -1), shift(second, 1)], axis=dim)


def expert_block(rows, gate_w, up_w, down_w):
    gate = jnp.dot(rows, gate_w, preferred_element_type=F32)
    upward = jnp.dot(rows, up_w, preferred_element_type=F32)
    activated = clamped_unit(gate, upward).astype(BF16)
    return jnp.dot(activated, down_w, preferred_element_type=F32).astype(BF16)


def exchange(x):
    return lax.all_to_all(x, EP, split_axis=0, concat_axis=0, tiled=True)


def shards(
    state_probe_logits,
    retention_logits,
    state_source_entries,
    state_result_switch_logits,
    retention_bound_margin,
    extra_fading_amount,
    state_result_scale,
    state_result_matrix,
    second_slice_tokens,
    specialist_assignment,
    selected_specialist_share,
    leading_scale_vector,
    trailing_scale_vector,
    specialist_switch_matrix,
    specialist_widen_matrix,
    specialist_contract_matrix,
):
    total_rows, width = state_probe_logits.shape
    members = lax.axis_size(EP)
    place = lax.axis_index("tp")
    ring = lax.axis_size("tp")
    features = second_slice_tokens.shape[1]

    own_route = lax.dynamic_slice_in_dim(specialist_assignment, place * TOK_DEV, TOK_DEV, 0)
    own_share = lax.dynamic_slice_in_dim(selected_specialist_share, place * TOK_DEV, TOK_DEV, 0)
    own_rows = lax.dynamic_slice_in_dim(second_slice_tokens, place * TOK_DEV, TOK_DEV, 0)
    normed = rms_scale(own_rows.astype(F32), leading_scale_vector).astype(BF16)
    experts = specialist_switch_matrix.shape[0] * members
    capacity = 2 * TOK_DEV * own_route.shape[1] // experts
    expert_ids = jnp.arange(experts, dtype=jnp.int32)[:, None]
    named = [(own_route[:, k][None, :] == expert_ids) for k in range(own_route.shape[1])]
    member = functools.reduce(jnp.logical_or, named)
    weight = sum(jnp.where(named[k], own_share[:, k][None, :], 0.0) for k in range(len(named)))
    ahead = jnp.arange(TOK_DEV)[:, None] < jnp.arange(TOK_DEV)[None, :]
    rank = jnp.dot(
        member.astype(BF16), ahead.astype(BF16), preferred_element_type=F32
    ).astype(jnp.int32)

    def slots_of(first, count):
        ids = first + jnp.arange(count, dtype=jnp.int32)
        return member[:, None, :] & (rank[:, None, :] == ids[None, :, None])

    pick = slots_of(0, capacity).astype(BF16).reshape(experts * capacity, TOK_DEV)
    packed = jnp.dot(pick, normed, preferred_element_type=F32).astype(BF16)
    arrived = exchange(packed.reshape(experts, capacity, features))
    gate_w = widened(specialist_switch_matrix[0], 1)
    up_w = widened(specialist_widen_matrix[0], 1)
    down_w = widened(specialist_contract_matrix[0], 0)

    raw, qdec, ends = local_pass(
        state_probe_logits,
        retention_logits,
        state_source_entries,
        retention_bound_margin,
        extra_fading_amount,
    )
    ends, arrived = lax.optimization_barrier((ends, arrived))
    slices = exchange(ends.reshape(members, width // members, 2 * HEAD))
    entering = exchange(prefix_pass(slices).astype(BF16)).reshape(width, HEAD)
    rec = output_pass(raw, qdec, entering, state_result_switch_logits, state_result_scale)

    combined = jnp.zeros((TOK_DEV, features), F32)
    count = capacity // GROUPS
    n = members * count
    for k in range(GROUPS):
        first = k * count
        own = arrived[:, first : first + count].reshape(n, features)
        out = expert_block(jnp.concatenate([own, across(own)], axis=0), gate_w, up_w, down_w)
        finished = (out[:n].astype(F32) + across(out[n:]).astype(F32)).astype(BF16)
        if k == GROUPS - 1:
            finished, rec = lax.optimization_barrier((finished, rec))
        returned = exchange(finished.reshape(members, count, features))
        share = jnp.where(slots_of(first, count), weight[:, None, :], 0.0)
        share = share.reshape(experts * count, TOK_DEV)
        coarse = share.astype(BF16)
        fine = (share - coarse.astype(F32)).astype(BF16)
        flat = returned.reshape(n, features)
        for piece in (coarse, fine):
            combined = combined + lax.dot_general(
                piece, flat, (((0,), (0,)), ((), ())), preferred_element_type=F32
            )
    moe_out = rms_scale(combined, trailing_scale_vector).astype(BF16)

    own, left, right, far = ring_gather(rec)
    by_block = state_result_matrix.reshape(ring, width, -1)

    def columns(block, at):
        held = lax.dynamic_index_in_dim(by_block, lax.rem(place + at, ring), 0, keepdims=False)
        return jnp.dot(block, held, preferred_element_type=F32)

    mixed = columns(own, 0) + columns(left, ring - 1) + columns(right, 1) + columns(far, 2)
    mixer_out = mixed.astype(BF16)
    return (mixer_out, moe_out)


def solution(mesh):
    finer = Mesh(mesh.devices.reshape(8, 4, 2, mesh.shape["tp"]), ("ep_0", "ep_1", "ep_2", "tp"))
    placed = (
        P(EP, "tp"),
        P(EP, "tp"),
        P(EP, "tp"),
        P(EP, "tp"),
        P("tp"),
        P(EP, "tp"),
        P("tp"),
        P(None, "tp"),
        P(EP, None),
        P(EP, None),
        P(EP, None),
        P(),
        P(),
        P(EP, None, "tp"),
        P(EP, None, "tp"),
        P(EP, "tp", None),
    )
    return jax.shard_map(
        shards,
        mesh=finer,
        in_specs=placed,
        out_specs=(P(EP, "tp"), P(EP_TP, None)),
        check_vma=False,
    )
```

```python
import functools

import jax
import jax.numpy as jnp
from jax import lax
from jax.experimental import pallas as pl
from jax.experimental.pallas import tpu as pltpu
from jax.sharding import Mesh
from jax.sharding import PartitionSpec as P

HEAD = 128
SPAN = 128
TOK_DEV = 128
EP = ("ep_0", "ep_1", "ep_2")
EP_TP = ("ep_0", "ep_1", "ep_2", "tp")
GROUPS = 2
CHUNKS = 2


NORM_EPS = 1e-06
SWISH_ALPHA = 1.702
CLAMP_LIMIT = 7.0

F32 = jnp.float32
BF16 = jnp.bfloat16


def rms_scale(values, gain):
    return values * lax.rsqrt(jnp.mean(values * values, axis=-1, keepdims=True) + NORM_EPS) * gain


def log_one_minus(x):
    total = jnp.full_like(x, 1.0 / 9.0)
    for k in range(8, 0, -1):
        total = total * x + 1.0 / k
    return -(x * total)


def split3(x):
    hi = x.astype(BF16)
    rest = x - hi.astype(F32)
    mid = rest.astype(BF16)
    low = (rest - mid.astype(F32)).astype(BF16)
    return hi, mid, low


def local_kernel(q_ref, r_ref, v_ref, m_ref, fade_ref, raw_ref, qdec_ref, st_ref):
    rows, width = q_ref.shape
    heads = width // HEAD
    steps = rows // SPAN
    row = lax.broadcasted_iota(jnp.int32, (SPAN, SPAN), 0)
    col = lax.broadcasted_iota(jnp.int32, (SPAN, SPAN), 1)
    lower = row >= col
    tri = lower.astype(F32).astype(BF16)
    margin = m_ref[...]

    def step(n, carry):
        base, states = carry
        at = pl.ds(pl.multiple_of(n * SPAN, SPAN), SPAN)
        q = q_ref[at, :].astype(F32)
        q = q / (1.0 + jnp.exp(-q)) * HEAD ** (-0.5)
        key = margin / (1.0 + jnp.exp(r_ref[at, :].astype(F32)))
        value = v_ref[at, :]
        fade = fade_ref[at, :]
        fade = jnp.concatenate(
            [jnp.broadcast_to(fade[:, h : h + 1], (SPAN, HEAD)) for h in range(heads)], axis=1
        )
        decay = log_one_minus(key) + fade
        cumul = sum(
            jnp.dot(tri, piece, preferred_element_type=F32) for piece in reversed(split3(decay))
        )
        middle = cumul[SPAN // 2 - 1 : SPAN // 2, :]
        last = cumul[SPAN - 1 : SPAN, :]
        grow = jnp.exp(cumul - middle)
        q_mid = (q * grow).astype(BF16)
        k_mid = (key * jnp.exp(middle - cumul)).astype(BF16)
        q_start = (q * jnp.exp(cumul)).astype(BF16)
        k_end = (key * jnp.exp(last - cumul)).astype(BF16)
        qdec_ref[at, :] = (q * jnp.exp(cumul + base)).astype(BF16)
        block_decay = jnp.exp(last)
        after = []
        for h in range(heads):
            c = slice(h * HEAD, (h + 1) * HEAD)
            scores = lax.dot_general(
                q_mid[:, c], k_mid[:, c], (((1,), (1,)), ((), ())), preferred_element_type=F32
            )
            scores = jnp.where(lower, scores, 0.0).astype(BF16)
            inner = jnp.dot(scores, value[:, c], preferred_element_type=F32)
            outer = jnp.dot(q_start[:, c], states[h].astype(BF16), preferred_element_type=F32)
            raw_ref[at, c] = inner + outer
            update = lax.dot_general(
                k_end[:, c], value[:, c], (((0,), (0,)), ((), ())), preferred_element_type=F32
            )
            wide = jnp.transpose(jnp.broadcast_to(block_decay[:, c], (HEAD, HEAD)))
            after.append(wide * states[h] + update)
        return base + last, tuple(after)

    base, states = lax.fori_loop(
        0,
        steps,
        step,
        (jnp.zeros((1, width), F32), tuple(jnp.zeros((HEAD, HEAD), F32) for _ in range(heads))),
    )
    total = jnp.exp(base)
    for h in range(heads):
        c = slice(h * HEAD, (h + 1) * HEAD)
        st_ref[c, :HEAD] = states[h]
        st_ref[c, HEAD:] = jnp.transpose(jnp.broadcast_to(total[:, c], (HEAD, HEAD)))


def prefix_kernel(x_ref, out_ref):
    state = jnp.zeros(out_ref.shape[1:], F32)
    for i in range(x_ref.shape[0]):
        out_ref[i] = state
        state = x_ref[i, :, HEAD:] * state + x_ref[i, :, :HEAD]


def output_kernel(raw_ref, qdec_ref, e_ref, gate_ref, scale_ref, out_ref):
    rows, width = raw_ref.shape
    tile = 256

    def step(n, carry):
        at = pl.ds(pl.multiple_of(n * tile, tile), tile)
        for h in range(width // HEAD):
            c = slice(h * HEAD, (h + 1) * HEAD)
            raw = raw_ref[at, c] + jnp.dot(
                qdec_ref[at, c], e_ref[c, :], preferred_element_type=F32
            )
            normed = raw * lax.rsqrt(jnp.mean(raw * raw, axis=-1, keepdims=True) + NORM_EPS)
            gate = gate_ref[at, c].astype(F32)
            out_ref[at, c] = (
                normed * scale_ref[:, c] * (gate / (1.0 + jnp.exp(-gate)))
            ).astype(BF16)
        return carry

    lax.fori_loop(0, rows // tile, step, 0)


def vmem_call(kernel, outs, flops, bytes_accessed, transcendentals):
    return pl.pallas_call(
        kernel,
        out_shape=outs,
        cost_estimate=pl.CostEstimate(
            flops=flops, bytes_accessed=bytes_accessed, transcendentals=transcendentals
        ),
    )


def local_pass(q, r, v, margin, fade):
    rows, width = q.shape
    return vmem_call(
        local_kernel,
        (
            jax.ShapeDtypeStruct((rows, width), F32),
            jax.ShapeDtypeStruct((rows, width), BF16),
            jax.ShapeDtypeStruct((width, 2 * HEAD), F32),
        ),
        4_000_000_000,
        6 << 20,
        rows * width * 6,
    )(q, r, v, margin.reshape(1, width), fade)


def prefix_pass(x):
    return vmem_call(
        prefix_kernel,
        jax.ShapeDtypeStruct((x.shape[0], x.shape[1], HEAD), F32),
        100_000_000,
        1 << 19,
        0,
    )(x)


def output_pass(raw, qdec, entering, gate, scale):
    rows, width = raw.shape
    return vmem_call(
        output_kernel,
        jax.ShapeDtypeStruct((rows, width), BF16),
        2_000_000_000,
        4 << 20,
        rows * width * 2,
    )(raw, qdec, entering, gate, scale.reshape(1, width))


def shift(x, by):
    n = lax.axis_size("tp")
    return lax.ppermute(x, "tp", [(i, (i + by) % n) for i in range(n)])


def expert_kernel(
    own_ref,
    far_ref,
    gate_own,
    gate_right,
    gate_left,
    up_own,
    up_right,
    up_left,
    down_own,
    down_right,
    down_left,
    out_own_ref,
    out_far_ref,
    rows,
    gate_w,
    up_w,
    down_w,
    hidden,
    sems,
):
    n = own_ref.shape[0]
    half = gate_right.shape[1]
    units = gate_w.shape[1]
    tile = half
    places = (slice(0, 2 * half), slice(2 * half, 3 * half), slice(3 * half, 4 * half))
    loads = []
    for k, place in enumerate(places):
        gate_src = (gate_own, gate_right, gate_left)[k]
        up_src = (up_own, up_right, up_left)[k]
        loads.append(pltpu.make_async_copy(gate_src, gate_w.at[:, place], sems.at[2 * k]))
        loads.append(pltpu.make_async_copy(up_src, up_w.at[:, place], sems.at[2 * k + 1]))
    for k, place in enumerate(places):
        down_src = (down_own, down_right, down_left)[k]
        loads.append(pltpu.make_async_copy(down_src, down_w.at[place, :], sems.at[6 + k]))
    for load in loads:
        load.start()
    rows[:n, :] = own_ref[...]
    rows[n:, :] = far_ref[...]

    def hidden_tile(f, carry):
        for first, k in ((0, 0), (2, 1), (3, 2)):

            @pl.when(f == first)
            def _():
                loads[2 * k].wait()
                loads[2 * k + 1].wait()

        at = pl.ds(pl.multiple_of(f * tile, tile), tile)
        gate = jnp.dot(rows[...], gate_w[:, at], preferred_element_type=F32)
        upward = jnp.dot(rows[...], up_w[:, at], preferred_element_type=F32)
        glued = jnp.minimum(gate, CLAMP_LIMIT)
        linear = jnp.clip(upward, -CLAMP_LIMIT, CLAMP_LIMIT)
        act = glued / (1.0 + jnp.exp(-SWISH_ALPHA * glued)) * (linear + 1.0)
        hidden[:, at] = act.astype(BF16)
        return carry

    lax.fori_loop(0, units // tile, hidden_tile, 0)
    for load in loads[6:]:
        load.wait()

    def out_tile(t, carry):
        at = pl.ds(pl.multiple_of(t * 512, 512), 512)
        part = jnp.dot(hidden[...], down_w[:, at], preferred_element_type=F32).astype(BF16)
        out_own_ref[:, at] = part[:n]
        out_far_ref[:, at] = part[n:]
        return carry

    lax.fori_loop(0, down_w.shape[1] // 512, out_tile, 0)


def expert_block(own, far, gates, ups, downs):
    n, features = own.shape
    units = sum(w.shape[1] for w in gates)
    vmem = pl.BlockSpec(memory_space=pltpu.VMEM)
    return pl.pallas_call(
        expert_kernel,
        out_shape=[jax.ShapeDtypeStruct((n, features), BF16)] * 2,
        in_specs=[vmem] * 2 + [pl.BlockSpec(memory_space=pl.ANY)] * 9,
        out_specs=[vmem] * 2,
        scratch_shapes=[
            pltpu.VMEM((2 * n, features), BF16),
            pltpu.VMEM((features, units), BF16),
            pltpu.VMEM((features, units), BF16),
            pltpu.VMEM((units, features), BF16),
            pltpu.VMEM((2 * n, units), BF16),
            pltpu.SemaphoreType.DMA((9,)),
        ],
        cost_estimate=pl.CostEstimate(
            flops=12 * n * features * units,
            bytes_accessed=6 * features * units + 8 * n * features,
            transcendentals=2 * n * units,
        ),
        name="expert_block",
    )(own, far, *gates, *ups, *downs)


def halves(weight, dim):
    half = weight.shape[dim] // 2
    return (
        lax.slice_in_dim(weight, 0, half, axis=dim),
        lax.slice_in_dim(weight, half, 2 * half, axis=dim),
    )


def widened(weight, pieces):
    first, second = pieces
    return weight, shift(first, -1), shift(second, 1)


def exchange(x):
    return lax.all_to_all(x, EP, split_axis=0, concat_axis=0, tiled=True)


def shards(
    state_probe_logits,
    retention_logits,
    state_source_entries,
    state_result_switch_logits,
    retention_bound_margin,
    extra_fading_amount,
    state_result_scale,
    state_result_matrix,
    second_slice_tokens,
    specialist_assignment,
    selected_specialist_share,
    leading_scale_vector,
    trailing_scale_vector,
    specialist_switch_matrix,
    specialist_widen_matrix,
    specialist_contract_matrix,
):
    _, width = state_probe_logits.shape
    members = lax.axis_size(EP)
    place = lax.axis_index("tp")
    ring = lax.axis_size("tp")
    features = second_slice_tokens.shape[1]

    own_route = lax.dynamic_slice_in_dim(specialist_assignment, place * TOK_DEV, TOK_DEV, 0)
    own_share = lax.dynamic_slice_in_dim(selected_specialist_share, place * TOK_DEV, TOK_DEV, 0)
    own_rows = lax.dynamic_slice_in_dim(second_slice_tokens, place * TOK_DEV, TOK_DEV, 0)

    gate_halves = halves(specialist_switch_matrix[0], 1)
    gate_halves, own_rows = lax.optimization_barrier((gate_halves, own_rows))
    gates = widened(specialist_switch_matrix[0], gate_halves)
    ups = widened(specialist_widen_matrix[0], halves(specialist_widen_matrix[0], 1))
    down_halves = halves(specialist_contract_matrix[0], 0)
    down_halves, retention_logits = lax.optimization_barrier((down_halves, retention_logits))
    downs = widened(specialist_contract_matrix[0], down_halves)
    normed = rms_scale(own_rows.astype(F32), leading_scale_vector).astype(BF16)
    experts = specialist_switch_matrix.shape[0] * members
    capacity = 2 * TOK_DEV * own_route.shape[1] // experts
    expert_ids = jnp.arange(experts, dtype=jnp.int32)[:, None]
    named = [(own_route[:, k][None, :] == expert_ids) for k in range(own_route.shape[1])]
    member = functools.reduce(jnp.logical_or, named)
    weight = sum(jnp.where(named[k], own_share[:, k][None, :], 0.0) for k in range(len(named)))
    ahead = jnp.arange(TOK_DEV)[:, None] < jnp.arange(TOK_DEV)[None, :]
    rank = jnp.dot(
        member.astype(BF16), ahead.astype(BF16), preferred_element_type=F32
    ).astype(jnp.int32)

    def slots_of(first, count):
        ids = first + jnp.arange(count, dtype=jnp.int32)
        return member[:, None, :] & (rank[:, None, :] == ids[None, :, None])

    pick = slots_of(0, capacity).astype(BF16).reshape(experts * capacity, TOK_DEV)
    packed = jnp.dot(pick, normed, preferred_element_type=F32).astype(BF16)
    arrived = exchange(packed.reshape(experts, capacity, features))

    raw, qdec, ends = local_pass(
        state_probe_logits,
        retention_logits,
        state_source_entries,
        retention_bound_margin,
        extra_fading_amount,
    )
    ends, arrived = lax.optimization_barrier((ends, arrived))
    slices = exchange(ends.reshape(members, width // members, 2 * HEAD))
    entering = exchange(prefix_pass(slices).astype(BF16)).reshape(width, HEAD)
    rec = output_pass(raw, qdec, entering, state_result_switch_logits, state_result_scale)

    combined = jnp.zeros((TOK_DEV, features), F32)
    count = capacity // GROUPS
    n = members * count // CHUNKS
    done = None
    for k in range(GROUPS):
        first = k * count
        group = arrived[:, first : first + count].reshape(CHUNKS * n, features)
        if done is not None:
            group, done = lax.optimization_barrier((group, done))
        owns = [group[c * n : (c + 1) * n] for c in range(CHUNKS)]
        fars = [shift(own, 2) for own in owns]
        parts = [expert_block(own, far, gates, ups, downs) for own, far in zip(owns, fars)]
        done = parts[-1][1]
        finished = [
            (mine.astype(F32) + shift(other, 2).astype(F32)).astype(BF16) for mine, other in parts
        ]
        finished = jnp.concatenate(finished, axis=0)
        if k == GROUPS - 1:
            finished, rec = lax.optimization_barrier((finished, rec))
        returned = exchange(finished.reshape(members, count, features))
        share = jnp.where(slots_of(first, count), weight[:, None, :], 0.0)
        share = share.reshape(experts * count, TOK_DEV)
        coarse = share.astype(BF16)
        fine = (share - coarse.astype(F32)).astype(BF16)
        flat = returned.reshape(members * count, features)
        for piece in (coarse, fine):
            combined = combined + lax.dot_general(
                piece, flat, (((0,), (0,)), ((), ())), preferred_element_type=F32
            )
    moe_out = rms_scale(combined, trailing_scale_vector).astype(BF16)

    own, left, right, far = rec, shift(rec, 1), shift(rec, -1), shift(rec, 2)
    by_block = state_result_matrix.reshape(ring, width, -1)

    def columns(block, at):
        held = lax.dynamic_index_in_dim(by_block, lax.rem(place + at, ring), 0, keepdims=False)
        return jnp.dot(block, held, preferred_element_type=F32)

    mixed = columns(own, 0) + columns(left, ring - 1) + columns(right, 1) + columns(far, 2)
    mixer_out = mixed.astype(BF16)
    return (mixer_out, moe_out)


def solution(mesh):
    finer = Mesh(mesh.devices.reshape(8, 4, 2, mesh.shape["tp"]), ("ep_0", "ep_1", "ep_2", "tp"))
    placed = (
        P(EP, "tp"),
        P(EP, "tp"),
        P(EP, "tp"),
        P(EP, "tp"),
        P("tp"),
        P(EP, "tp"),
        P("tp"),
        P(None, "tp"),
        P(EP, None),
        P(EP, None),
        P(EP, None),
        P(),
        P(),
        P(EP, None, "tp"),
        P(EP, None, "tp"),
        P(EP, "tp", None),
    )

    return jax.shard_map(
        shards,
        mesh=finer,
        in_specs=placed,
        out_specs=(P(EP, "tp"), P(EP_TP, None)),
        check_vma=False,
    )
```

```python
import functools

import jax
import jax.numpy as jnp
from jax import lax
from jax.experimental import pallas as pl
from jax.experimental.pallas import tpu as pltpu
from jax.sharding import Mesh
from jax.sharding import PartitionSpec as P

HEAD = 128
SPAN = 128
TOK_DEV = 128
EP = ("ep_0", "ep_1", "ep_2")
EP_TP = ("ep_0", "ep_1", "ep_2", "tp")
GROUPS = 2
EXPERT_VMEM = 24 << 20
SMALL_VMEM = 12 << 20
CHUNKS = 2


NORM_EPS = 1e-06
SWISH_ALPHA = 1.702
CLAMP_LIMIT = 7.0

F32 = jnp.float32
BF16 = jnp.bfloat16


def rms_scale(values, gain):
    return values * lax.rsqrt(jnp.mean(values * values, axis=-1, keepdims=True) + NORM_EPS) * gain


def log_one_minus(x):
    total = jnp.full_like(x, 1.0 / 9.0)
    for k in range(8, 0, -1):
        total = total * x + 1.0 / k
    return -(x * total)


def split3(x):
    hi = x.astype(BF16)
    rest = x - hi.astype(F32)
    mid = rest.astype(BF16)
    low = (rest - mid.astype(F32)).astype(BF16)
    return hi, mid, low


def local_kernel(q_ref, r_ref, v_ref, m_ref, fade_ref, raw_ref, qdec_ref, st_ref):
    rows, width = q_ref.shape
    heads = width // HEAD
    steps = rows // SPAN
    row = lax.broadcasted_iota(jnp.int32, (SPAN, SPAN), 0)
    col = lax.broadcasted_iota(jnp.int32, (SPAN, SPAN), 1)
    lower = row >= col
    tri = lower.astype(F32).astype(BF16)
    margin = m_ref[...]

    def step(n, carry):
        base, states = carry
        at = pl.ds(pl.multiple_of(n * SPAN, SPAN), SPAN)
        q = q_ref[at, :].astype(F32)
        q = q / (1.0 + jnp.exp(-q)) * HEAD ** (-0.5)
        key = margin / (1.0 + jnp.exp(r_ref[at, :].astype(F32)))
        value = v_ref[at, :]
        fade = fade_ref[at, :]
        fade = jnp.concatenate(
            [jnp.broadcast_to(fade[:, h : h + 1], (SPAN, HEAD)) for h in range(heads)], axis=1
        )
        decay = log_one_minus(key) + fade
        cumul = sum(
            jnp.dot(tri, piece, preferred_element_type=F32) for piece in reversed(split3(decay))
        )
        middle = cumul[SPAN // 2 - 1 : SPAN // 2, :]
        last = cumul[SPAN - 1 : SPAN, :]
        grow = jnp.exp(cumul - middle)
        q_mid = (q * grow).astype(BF16)
        k_mid = (key * jnp.exp(middle - cumul)).astype(BF16)
        q_start = (q * jnp.exp(cumul)).astype(BF16)
        k_end = (key * jnp.exp(last - cumul)).astype(BF16)
        qdec_ref[at, :] = (q * jnp.exp(cumul + base)).astype(BF16)
        block_decay = jnp.exp(last)
        after = []
        for h in range(heads):
            c = slice(h * HEAD, (h + 1) * HEAD)
            scores = lax.dot_general(
                q_mid[:, c], k_mid[:, c], (((1,), (1,)), ((), ())), preferred_element_type=F32
            )
            scores = jnp.where(lower, scores, 0.0).astype(BF16)
            inner = jnp.dot(scores, value[:, c], preferred_element_type=F32)
            outer = jnp.dot(q_start[:, c], states[h].astype(BF16), preferred_element_type=F32)
            raw_ref[at, c] = inner + outer
            update = lax.dot_general(
                k_end[:, c], value[:, c], (((0,), (0,)), ((), ())), preferred_element_type=F32
            )
            wide = jnp.transpose(jnp.broadcast_to(block_decay[:, c], (HEAD, HEAD)))
            after.append(wide * states[h] + update)
        return base + last, tuple(after)

    base, states = lax.fori_loop(
        0,
        steps,
        step,
        (jnp.zeros((1, width), F32), tuple(jnp.zeros((HEAD, HEAD), F32) for _ in range(heads))),
    )
    total = jnp.exp(base)
    for h in range(heads):
        c = slice(h * HEAD, (h + 1) * HEAD)
        st_ref[c, :HEAD] = states[h]
        st_ref[c, HEAD:] = jnp.transpose(jnp.broadcast_to(total[:, c], (HEAD, HEAD)))


def prefix_kernel(x_ref, out_ref):
    state = jnp.zeros(out_ref.shape[1:], F32)
    for i in range(x_ref.shape[0]):
        out_ref[i] = state
        state = x_ref[i, :, HEAD:] * state + x_ref[i, :, :HEAD]


def output_kernel(raw_ref, qdec_ref, e_ref, gate_ref, scale_ref, out_ref):
    rows, width = raw_ref.shape
    tile = 256

    def step(n, carry):
        at = pl.ds(pl.multiple_of(n * tile, tile), tile)
        for h in range(width // HEAD):
            c = slice(h * HEAD, (h + 1) * HEAD)
            raw = raw_ref[at, c] + jnp.dot(
                qdec_ref[at, c], e_ref[c, :], preferred_element_type=F32
            )
            normed = raw * lax.rsqrt(jnp.mean(raw * raw, axis=-1, keepdims=True) + NORM_EPS)
            gate = gate_ref[at, c].astype(F32)
            out_ref[at, c] = (
                normed * scale_ref[:, c] * (gate / (1.0 + jnp.exp(-gate)))
            ).astype(BF16)
        return carry

    lax.fori_loop(0, rows // tile, step, 0)


def vmem_call(kernel, outs, flops, bytes_accessed, transcendentals):
    return pl.pallas_call(
        kernel,
        out_shape=outs,
        compiler_params=pltpu.CompilerParams(vmem_limit_bytes=SMALL_VMEM),
        cost_estimate=pl.CostEstimate(
            flops=flops, bytes_accessed=bytes_accessed, transcendentals=transcendentals
        ),
    )


def local_pass(q, r, v, margin, fade):
    rows, width = q.shape
    return vmem_call(
        local_kernel,
        (
            jax.ShapeDtypeStruct((rows, width), F32),
            jax.ShapeDtypeStruct((rows, width), BF16),
            jax.ShapeDtypeStruct((width, 2 * HEAD), F32),
        ),
        4_000_000_000,
        6 << 20,
        rows * width * 6,
    )(q, r, v, margin.reshape(1, width), fade)


def prefix_pass(x):
    return vmem_call(
        prefix_kernel,
        jax.ShapeDtypeStruct((x.shape[0], x.shape[1], HEAD), F32),
        100_000_000,
        1 << 19,
        0,
    )(x)


def output_pass(raw, qdec, entering, gate, scale):
    rows, width = raw.shape
    return vmem_call(
        output_kernel,
        jax.ShapeDtypeStruct((rows, width), BF16),
        2_000_000_000,
        4 << 20,
        rows * width * 2,
    )(raw, qdec, entering, gate, scale.reshape(1, width))


def shift(x, by):
    n = lax.axis_size("tp")
    return lax.ppermute(x, "tp", [(i, (i + by) % n) for i in range(n)])


def expert_kernel(
    own_ref,
    far_ref,
    gate_own,
    gate_right,
    gate_left,
    up_own,
    up_right,
    up_left,
    down_own,
    down_right,
    down_left,
    out_own_ref,
    out_far_ref,
    rows,
    hidden,
    gate_more,
    up_more,
    down_more,
    sems,
):
    n = own_ref.shape[0]
    tile = gate_right.shape[1]
    first, second = slice(0, tile), slice(tile, 2 * tile)
    loads = [
        pltpu.make_async_copy(gate_right, gate_more.at[:, first], sems.at[0]),
        pltpu.make_async_copy(gate_left, gate_more.at[:, second], sems.at[1]),
        pltpu.make_async_copy(up_right, up_more.at[:, first], sems.at[2]),
        pltpu.make_async_copy(up_left, up_more.at[:, second], sems.at[3]),
        pltpu.make_async_copy(down_right, down_more.at[first, :], sems.at[4]),
        pltpu.make_async_copy(down_left, down_more.at[second, :], sems.at[5]),
    ]
    for load in loads:
        load.start()
    rows[:n, :] = own_ref[...]
    rows[n:, :] = far_ref[...]

    def hidden_tiles(gate_w, up_w, offset):
        def step(f, carry):
            at = pl.ds(pl.multiple_of(f * tile, tile), tile)
            to = pl.ds(pl.multiple_of(f * tile + offset, tile), tile)
            gate = jnp.dot(rows[...], gate_w[:, at], preferred_element_type=F32)
            upward = jnp.dot(rows[...], up_w[:, at], preferred_element_type=F32)
            glued = jnp.minimum(gate, CLAMP_LIMIT)
            linear = jnp.clip(upward, -CLAMP_LIMIT, CLAMP_LIMIT)
            act = glued / (1.0 + jnp.exp(-SWISH_ALPHA * glued)) * (linear + 1.0)
            hidden[:, to] = act.astype(BF16)
            return carry

        lax.fori_loop(0, 2, step, 0)

    hidden_tiles(gate_own, up_own, 0)
    for load in loads[:4]:
        load.wait()
    hidden_tiles(gate_more, up_more, 2 * tile)
    for load in loads[4:]:
        load.wait()

    def out_tile(t, carry):
        at = pl.ds(pl.multiple_of(t * 256, 256), 256)
        part = (
            jnp.dot(hidden[:, : 2 * tile], down_own[:, at], preferred_element_type=F32)
            + jnp.dot(hidden[:, 2 * tile :], down_more[:, at], preferred_element_type=F32)
        ).astype(BF16)
        out_own_ref[:, at] = part[:n]
        out_far_ref[:, at] = part[n:]
        return carry

    lax.fori_loop(0, down_own.shape[1] // 256, out_tile, 0)


def expert_block(own, far, gates, ups, downs):
    n, features = own.shape
    units = sum(w.shape[1] for w in gates)
    vmem = pl.BlockSpec(memory_space=pltpu.VMEM)
    hbm = pl.BlockSpec(memory_space=pltpu.HBM)
    half = units // 2
    return pl.pallas_call(
        expert_kernel,
        out_shape=[jax.ShapeDtypeStruct((n, features), BF16)] * 2,
        in_specs=[vmem] * 2 + [vmem, hbm, hbm] * 3,
        out_specs=[vmem] * 2,
        scratch_shapes=[
            pltpu.VMEM((2 * n, features), BF16),
            pltpu.VMEM((2 * n, units), BF16),
            pltpu.VMEM((features, half), BF16),
            pltpu.VMEM((features, half), BF16),
            pltpu.VMEM((half, features), BF16),
            pltpu.SemaphoreType.DMA((6,)),
        ],
        compiler_params=pltpu.CompilerParams(vmem_limit_bytes=EXPERT_VMEM),
        cost_estimate=pl.CostEstimate(
            flops=12 * n * features * units,
            bytes_accessed=6 * features * units + 8 * n * features,
            transcendentals=2 * n * units,
        ),
        name="expert_block",
    )(own, far, *gates, *ups, *downs)


def halves(weight, dim):
    half = weight.shape[dim] // 2
    return (
        lax.slice_in_dim(weight, 0, half, axis=dim),
        lax.slice_in_dim(weight, half, 2 * half, axis=dim),
    )


def widened(weight, pieces):
    first, second = pieces
    return weight, shift(first, -1), shift(second, 1)


def exchange(x):
    return lax.all_to_all(x, EP, split_axis=0, concat_axis=0, tiled=True)


def shards(
    state_probe_logits,
    retention_logits,
    state_source_entries,
    state_result_switch_logits,
    retention_bound_margin,
    extra_fading_amount,
    state_result_scale,
    state_result_matrix,
    second_slice_tokens,
    specialist_assignment,
    selected_specialist_share,
    leading_scale_vector,
    trailing_scale_vector,
    specialist_switch_matrix,
    specialist_widen_matrix,
    specialist_contract_matrix,
):
    _, width = state_probe_logits.shape
    members = lax.axis_size(EP)
    place = lax.axis_index("tp")
    ring = lax.axis_size("tp")
    features = second_slice_tokens.shape[1]

    own_route = lax.dynamic_slice_in_dim(specialist_assignment, place * TOK_DEV, TOK_DEV, 0)
    own_share = lax.dynamic_slice_in_dim(selected_specialist_share, place * TOK_DEV, TOK_DEV, 0)
    own_rows = lax.dynamic_slice_in_dim(second_slice_tokens, place * TOK_DEV, TOK_DEV, 0)

    gate_halves = halves(specialist_switch_matrix[0], 1)
    gate_halves, own_rows = lax.optimization_barrier((gate_halves, own_rows))
    gates = widened(specialist_switch_matrix[0], gate_halves)
    ups = widened(specialist_widen_matrix[0], halves(specialist_widen_matrix[0], 1))
    down_halves = halves(specialist_contract_matrix[0], 0)
    down_halves, retention_logits = lax.optimization_barrier((down_halves, retention_logits))
    downs = widened(specialist_contract_matrix[0], down_halves)
    normed = rms_scale(own_rows.astype(F32), leading_scale_vector).astype(BF16)
    experts = specialist_switch_matrix.shape[0] * members
    capacity = 2 * TOK_DEV * own_route.shape[1] // experts
    expert_ids = jnp.arange(experts, dtype=jnp.int32)[:, None]
    named = [(own_route[:, k][None, :] == expert_ids) for k in range(own_route.shape[1])]
    member = functools.reduce(jnp.logical_or, named)
    weight = sum(jnp.where(named[k], own_share[:, k][None, :], 0.0) for k in range(len(named)))
    ahead = jnp.arange(TOK_DEV)[:, None] < jnp.arange(TOK_DEV)[None, :]
    rank = jnp.dot(
        member.astype(BF16), ahead.astype(BF16), preferred_element_type=F32
    ).astype(jnp.int32)

    def slots_of(first, count):
        ids = first + jnp.arange(count, dtype=jnp.int32)
        return member[:, None, :] & (rank[:, None, :] == ids[None, :, None])

    pick = slots_of(0, capacity).astype(BF16).reshape(experts * capacity, TOK_DEV)
    packed = jnp.dot(pick, normed, preferred_element_type=F32).astype(BF16)
    arrived = exchange(packed.reshape(experts, capacity, features))

    raw, qdec, ends = local_pass(
        state_probe_logits,
        retention_logits,
        state_source_entries,
        retention_bound_margin,
        extra_fading_amount,
    )
    ends = ends.reshape(members, width // members, 2 * HEAD)
    ends, arrived = lax.optimization_barrier((ends, arrived))
    slices = exchange(ends)

    combined = jnp.zeros((TOK_DEV, features), F32)
    count = capacity // GROUPS
    n = members * count // CHUNKS
    flat_in = arrived.reshape(CHUNKS, -1, features)
    at = jnp.arange(n, dtype=jnp.int32)
    where = at // count * capacity + at % count
    owns = []
    for k in range(GROUPS):
        chosen = (where + k * count)[:, None] == jnp.arange(flat_in.shape[1])[None, :]
        for c in range(CHUNKS):
            owns.append(
                jnp.dot(chosen.astype(BF16), flat_in[c], preferred_element_type=F32).astype(BF16)
            )
    parts = []
    for k in range(GROUPS):
        for c in range(CHUNKS):
            i = k * CHUNKS + c
            own = owns[i]
            if i >= 3:
                own, gate = lax.optimization_barrier((own, parts[i - 2][1]))
                parts[i - 2] = (parts[i - 2][0], gate)
            far = shift(own, 2)
            parts.append(expert_block(own, far, gates, ups, downs))
            if i == 1:
                entering = exchange(prefix_pass(slices).astype(BF16)).reshape(width, HEAD)
    rec = output_pass(raw, qdec, entering, state_result_switch_logits, state_result_scale)
    parts[-1], rec = lax.optimization_barrier((parts[-1], rec))
    for k in range(GROUPS):
        first = k * count
        finished = []
        for c in range(CHUNKS):
            mine, other = parts[k * CHUNKS + c]
            back = shift(other, 2)
            finished.append((mine.astype(F32) + back.astype(F32)).astype(BF16))
        finished = jnp.concatenate(finished, axis=0)
        returned = exchange(finished.reshape(members, count, features))
        share = jnp.where(slots_of(first, count), weight[:, None, :], 0.0)
        share = share.reshape(experts * count, TOK_DEV)
        coarse = share.astype(BF16)
        fine = (share - coarse.astype(F32)).astype(BF16)
        flat = returned.reshape(members * count, features)
        for piece in (coarse, fine):
            combined = combined + lax.dot_general(
                piece, flat, (((0,), (0,)), ((), ())), preferred_element_type=F32
            )
    moe_out = rms_scale(combined, trailing_scale_vector).astype(BF16)

    own, left, right, far = rec, shift(rec, 1), shift(rec, -1), shift(rec, 2)
    by_block = state_result_matrix.reshape(ring, width, -1)

    def columns(block, at):
        held = lax.dynamic_index_in_dim(by_block, lax.rem(place + at, ring), 0, keepdims=False)
        return jnp.dot(block, held, preferred_element_type=F32)

    mixed = columns(own, 0) + columns(left, ring - 1) + columns(right, 1) + columns(far, 2)
    mixer_out = mixed.astype(BF16)
    return (mixer_out, moe_out)


def solution(mesh):
    finer = Mesh(mesh.devices.reshape(8, 4, 2, mesh.shape["tp"]), ("ep_0", "ep_1", "ep_2", "tp"))
    placed = (
        P(EP, "tp"),
        P(EP, "tp"),
        P(EP, "tp"),
        P(EP, "tp"),
        P("tp"),
        P(EP, "tp"),
        P("tp"),
        P(None, "tp"),
        P(EP, None),
        P(EP, None),
        P(EP, None),
        P(),
        P(),
        P(EP, None, "tp"),
        P(EP, None, "tp"),
        P(EP, "tp", None),
    )

    return jax.shard_map(
        shards,
        mesh=finer,
        in_specs=placed,
        out_specs=(P(EP, "tp"), P(EP_TP, None)),
        check_vma=False,
    )
```

```python
import functools

import jax
import jax.numpy as jnp
from jax import lax
from jax.experimental import pallas as pl
from jax.experimental.pallas import tpu as pltpu
from jax.sharding import Mesh
from jax.sharding import PartitionSpec as P

HEAD = 128
SPAN = 128
TOK_DEV = 128
EP = ("ep_0", "ep_1", "ep_2")
EP_TP = ("ep_0", "ep_1", "ep_2", "tp")
GROUPS = 2
CHUNKS = 2


NORM_EPS = 1e-06
SWISH_ALPHA = 1.702
CLAMP_LIMIT = 7.0

F32 = jnp.float32
BF16 = jnp.bfloat16


def rms_scale(values, gain):
    return values * lax.rsqrt(jnp.mean(values * values, axis=-1, keepdims=True) + NORM_EPS) * gain


def log_one_minus(x):
    total = jnp.full_like(x, 1.0 / 9.0)
    for k in range(8, 0, -1):
        total = total * x + 1.0 / k
    return -(x * total)


def split3(x):
    hi = x.astype(BF16)
    rest = x - hi.astype(F32)
    mid = rest.astype(BF16)
    low = (rest - mid.astype(F32)).astype(BF16)
    return hi, mid, low


def local_kernel(q_ref, r_ref, v_ref, m_ref, fade_ref, raw_ref, qdec_ref, st_ref):
    rows, width = q_ref.shape
    heads = width // HEAD
    steps = rows // SPAN
    row = lax.broadcasted_iota(jnp.int32, (SPAN, SPAN), 0)
    col = lax.broadcasted_iota(jnp.int32, (SPAN, SPAN), 1)
    lower = row >= col
    tri = lower.astype(F32).astype(BF16)
    margin = m_ref[...]

    def step(n, carry):
        base, states = carry
        at = pl.ds(pl.multiple_of(n * SPAN, SPAN), SPAN)
        q = q_ref[at, :].astype(F32)
        q = q / (1.0 + jnp.exp(-q)) * HEAD ** (-0.5)
        key = margin / (1.0 + jnp.exp(r_ref[at, :].astype(F32)))
        value = v_ref[at, :]
        fade = fade_ref[at, :]
        fade = jnp.concatenate(
            [jnp.broadcast_to(fade[:, h : h + 1], (SPAN, HEAD)) for h in range(heads)], axis=1
        )
        decay = log_one_minus(key) + fade
        cumul = sum(
            jnp.dot(tri, piece, preferred_element_type=F32) for piece in reversed(split3(decay))
        )
        middle = cumul[SPAN // 2 - 1 : SPAN // 2, :]
        last = cumul[SPAN - 1 : SPAN, :]
        grow = jnp.exp(cumul - middle)
        q_mid = (q * grow).astype(BF16)
        k_mid = (key * jnp.exp(middle - cumul)).astype(BF16)
        q_start = (q * jnp.exp(cumul)).astype(BF16)
        k_end = (key * jnp.exp(last - cumul)).astype(BF16)
        qdec_ref[at, :] = (q * jnp.exp(cumul + base)).astype(BF16)
        block_decay = jnp.exp(last)
        after = []
        for h in range(heads):
            c = slice(h * HEAD, (h + 1) * HEAD)
            scores = lax.dot_general(
                q_mid[:, c], k_mid[:, c], (((1,), (1,)), ((), ())), preferred_element_type=F32
            )
            scores = jnp.where(lower, scores, 0.0).astype(BF16)
            inner = jnp.dot(scores, value[:, c], preferred_element_type=F32)
            outer = jnp.dot(q_start[:, c], states[h].astype(BF16), preferred_element_type=F32)
            raw_ref[at, c] = inner + outer
            update = lax.dot_general(
                k_end[:, c], value[:, c], (((0,), (0,)), ((), ())), preferred_element_type=F32
            )
            wide = jnp.transpose(jnp.broadcast_to(block_decay[:, c], (HEAD, HEAD)))
            after.append(wide * states[h] + update)
        return base + last, tuple(after)

    base, states = lax.fori_loop(
        0,
        steps,
        step,
        (jnp.zeros((1, width), F32), tuple(jnp.zeros((HEAD, HEAD), F32) for _ in range(heads))),
    )
    total = jnp.exp(base)
    for h in range(heads):
        c = slice(h * HEAD, (h + 1) * HEAD)
        st_ref[c, :HEAD] = states[h]
        st_ref[c, HEAD:] = jnp.transpose(jnp.broadcast_to(total[:, c], (HEAD, HEAD)))


def prefix_kernel(x_ref, out_ref):
    state = jnp.zeros(out_ref.shape[1:], F32)
    for i in range(x_ref.shape[0]):
        out_ref[i] = state.astype(BF16)
        state = x_ref[i, :, HEAD:] * state + x_ref[i, :, :HEAD]


def output_kernel(raw_ref, qdec_ref, e_ref, gate_ref, scale_ref, out_ref):
    rows, width = raw_ref.shape
    tile = 256

    def step(n, carry):
        at = pl.ds(pl.multiple_of(n * tile, tile), tile)
        for h in range(width // HEAD):
            c = slice(h * HEAD, (h + 1) * HEAD)
            raw = raw_ref[at, c] + jnp.dot(
                qdec_ref[at, c], e_ref[c, :], preferred_element_type=F32
            )
            normed = raw * lax.rsqrt(jnp.mean(raw * raw, axis=-1, keepdims=True) + NORM_EPS)
            gate = gate_ref[at, c].astype(F32)
            out_ref[at, c] = (
                normed * scale_ref[:, c] * (gate / (1.0 + jnp.exp(-gate)))
            ).astype(BF16)
        return carry

    lax.fori_loop(0, rows // tile, step, 0)


def vmem_call(kernel, outs, flops, bytes_accessed, transcendentals):
    return pl.pallas_call(
        kernel,
        out_shape=outs,
        cost_estimate=pl.CostEstimate(
            flops=flops, bytes_accessed=bytes_accessed, transcendentals=transcendentals
        ),
    )


def local_pass(q, r, v, margin, fade):
    rows, width = q.shape
    return vmem_call(
        local_kernel,
        (
            jax.ShapeDtypeStruct((rows, width), F32),
            jax.ShapeDtypeStruct((rows, width), BF16),
            jax.ShapeDtypeStruct((width, 2 * HEAD), F32),
        ),
        4_000_000_000,
        6 << 20,
        rows * width * 6,
    )(q, r, v, margin.reshape(1, width), fade)


def prefix_pass(x):
    return vmem_call(
        prefix_kernel,
        jax.ShapeDtypeStruct((x.shape[0], x.shape[1], HEAD), BF16),
        100_000_000,
        1 << 19,
        0,
    )(x)


def output_pass(raw, qdec, entering, gate, scale):
    rows, width = raw.shape
    return vmem_call(
        output_kernel,
        jax.ShapeDtypeStruct((rows, width), BF16),
        2_000_000_000,
        4 << 20,
        rows * width * 2,
    )(raw, qdec, entering, gate, scale.reshape(1, width))


def shift(x, by):
    n = lax.axis_size("tp")
    return lax.ppermute(x, "tp", [(i, (i + by) % n) for i in range(n)])


def expert_kernel(
    own,
    far,
    gate_own,
    gate_right,
    gate_left,
    up_own,
    up_right,
    up_left,
    down_own,
    down_right,
    down_left,
    out_own,
    out_far,
    rows,
    gate_w,
    up_w,
    down_w,
    hidden,
    out,
    sems,
    out_sems,
):
    n = own.shape[0]
    tile = gate_right.shape[1]
    wide = 512
    tiles = gate_w.shape[1] // tile

    def columns(owned, right, left):
        return [owned.at[:, pl.ds(0, tile)], owned.at[:, pl.ds(tile, tile)], right, left]

    gates = columns(gate_own, gate_right, gate_left)
    ups = columns(up_own, up_right, up_left)
    downs = [down_own.at[pl.ds(0, tile), :], down_own.at[pl.ds(tile, tile), :]]
    downs += [down_right, down_left]
    places = [pl.ds(f * tile, tile) for f in range(tiles)]
    loads = [
        pltpu.make_async_copy(own, rows.at[pl.ds(0, n), :], sems.at[0]),
        pltpu.make_async_copy(far, rows.at[pl.ds(n, n), :], sems.at[1]),
    ]
    for f in range(tiles):
        loads.append(pltpu.make_async_copy(gates[f], gate_w.at[:, places[f]], sems.at[2 + 2 * f]))
        loads.append(pltpu.make_async_copy(ups[f], up_w.at[:, places[f]], sems.at[3 + 2 * f]))
    for f in range(tiles):
        to = down_w.at[places[f], :]
        loads.append(pltpu.make_async_copy(downs[f], to, sems.at[2 + 2 * tiles + f]))
    for load in loads:
        load.start()
    loads[0].wait()
    loads[1].wait()

    def hidden_tile(f, carry):
        for k in range(tiles):

            @pl.when(f == k)
            def _():
                loads[2 + 2 * k].wait()
                loads[3 + 2 * k].wait()

        at = pl.ds(pl.multiple_of(f * tile, tile), tile)
        gate = jnp.dot(rows[...], gate_w[:, at], preferred_element_type=F32)
        upward = jnp.dot(rows[...], up_w[:, at], preferred_element_type=F32)
        glued = jnp.minimum(gate, CLAMP_LIMIT)
        linear = jnp.clip(upward, -CLAMP_LIMIT, CLAMP_LIMIT)
        act = glued / (1.0 + jnp.exp(-SWISH_ALPHA * glued)) * (linear + 1.0)
        hidden[:, at] = act.astype(BF16)
        return carry

    lax.fori_loop(0, tiles, hidden_tile, 0)
    for load in loads[2 + 2 * tiles :]:
        load.wait()

    stores = []
    for t in range(out.shape[1] // wide):
        at = pl.ds(t * wide, wide)
        stores.append(
            (
                pltpu.make_async_copy(
                    out.at[pl.ds(0, n), at], out_own.at[:, at], out_sems.at[2 * t]
                ),
                pltpu.make_async_copy(
                    out.at[pl.ds(n, n), at], out_far.at[:, at], out_sems.at[2 * t + 1]
                ),
            )
        )

    def out_tile(t, carry):
        at = pl.ds(pl.multiple_of(t * wide, wide), wide)
        part = jnp.dot(hidden[...], down_w[:, at], preferred_element_type=F32)
        out[:, at] = part.astype(BF16)
        for k, pair in enumerate(stores):

            @pl.when(t == k)
            def _():
                for store in pair:
                    store.start()

        return carry

    lax.fori_loop(0, len(stores), out_tile, 0)
    for pair in stores:
        for store in pair:
            store.wait()


def expert_block(own, far, gates, ups, downs):
    n, features = own.shape
    units = sum(w.shape[1] for w in gates)
    hbm = pl.BlockSpec(memory_space=pltpu.HBM)
    return pl.pallas_call(
        expert_kernel,
        out_shape=[jax.ShapeDtypeStruct((n, features), BF16)] * 2,
        in_specs=[hbm] * 11,
        out_specs=[hbm] * 2,
        scratch_shapes=[
            pltpu.VMEM((2 * n, features), BF16),
            pltpu.VMEM((features, units), BF16),
            pltpu.VMEM((features, units), BF16),
            pltpu.VMEM((units, features), BF16),
            pltpu.VMEM((2 * n, units), BF16),
            pltpu.VMEM((2 * n, features), BF16),
            pltpu.SemaphoreType.DMA((14,)),
            pltpu.SemaphoreType.DMA((8,)),
        ],
        cost_estimate=pl.CostEstimate(
            flops=12 * n * features * units,
            bytes_accessed=6 * features * units + 8 * n * features,
            transcendentals=2 * n * units,
        ),
        name="expert_block",
    )(own, far, *gates, *ups, *downs)


def finish_kernel(flat_ref, coarse_ref, fine_ref, partial_ref, gain_ref, out_ref):
    total = partial_ref[...]
    for share in (coarse_ref, fine_ref):
        total = total + lax.dot_general(
            share[...], flat_ref[...], (((0,), (0,)), ((), ())), preferred_element_type=F32
        )
    out_ref[...] = rms_scale(total, gain_ref[...]).astype(BF16)


def finish(flat, coarse, fine, partial, gain):
    tokens, features = partial.shape
    return vmem_call(
        finish_kernel,
        jax.ShapeDtypeStruct((tokens, features), BF16),
        4 * flat.shape[0] * tokens * features,
        4 << 20,
        tokens,
    )(flat, coarse, fine, partial, gain.reshape(1, features))


def halves(weight, dim):
    half = weight.shape[dim] // 2
    return (
        lax.slice_in_dim(weight, 0, half, axis=dim),
        lax.slice_in_dim(weight, half, 2 * half, axis=dim),
    )


def widened(weight, pieces):
    first, second = pieces
    return weight, shift(first, -1), shift(second, 1)


def exchange(x):
    return lax.all_to_all(x, EP, split_axis=0, concat_axis=0, tiled=True)


def shards(
    state_probe_logits,
    retention_logits,
    state_source_entries,
    state_result_switch_logits,
    retention_bound_margin,
    extra_fading_amount,
    state_result_scale,
    state_result_matrix,
    second_slice_tokens,
    specialist_assignment,
    selected_specialist_share,
    leading_scale_vector,
    trailing_scale_vector,
    specialist_switch_matrix,
    specialist_widen_matrix,
    specialist_contract_matrix,
):
    _, width = state_probe_logits.shape
    members = lax.axis_size(EP)
    place = lax.axis_index("tp")
    ring = lax.axis_size("tp")
    features = second_slice_tokens.shape[1]

    own_route = lax.dynamic_slice_in_dim(specialist_assignment, place * TOK_DEV, TOK_DEV, 0)
    own_share = lax.dynamic_slice_in_dim(selected_specialist_share, place * TOK_DEV, TOK_DEV, 0)
    own_rows = lax.dynamic_slice_in_dim(second_slice_tokens, place * TOK_DEV, TOK_DEV, 0)

    down_halves = halves(specialist_contract_matrix[0], 0)
    down_halves, own_rows = lax.optimization_barrier((down_halves, own_rows))
    downs = widened(specialist_contract_matrix[0], down_halves)
    gates = widened(specialist_switch_matrix[0], halves(specialist_switch_matrix[0], 1))
    up_halves = halves(specialist_widen_matrix[0], 1)
    up_halves, retention_logits = lax.optimization_barrier((up_halves, retention_logits))
    ups = widened(specialist_widen_matrix[0], up_halves)
    normed = rms_scale(own_rows.astype(F32), leading_scale_vector).astype(BF16)
    experts = specialist_switch_matrix.shape[0] * members
    capacity = 2 * TOK_DEV * own_route.shape[1] // experts
    expert_ids = jnp.arange(experts, dtype=jnp.int32)[:, None]
    named = [(own_route[:, k][None, :] == expert_ids) for k in range(own_route.shape[1])]
    member = functools.reduce(jnp.logical_or, named)
    weight = sum(jnp.where(named[k], own_share[:, k][None, :], 0.0) for k in range(len(named)))
    ahead = jnp.arange(TOK_DEV)[:, None] < jnp.arange(TOK_DEV)[None, :]
    rank = jnp.dot(
        member.astype(BF16), ahead.astype(BF16), preferred_element_type=F32
    ).astype(jnp.int32)

    def slots_of(first, count):
        ids = first + jnp.arange(count, dtype=jnp.int32)
        return member[:, None, :] & (rank[:, None, :] == ids[None, :, None])

    pick = slots_of(0, capacity).astype(BF16).reshape(experts * capacity, TOK_DEV)
    packed = jnp.dot(pick, normed, preferred_element_type=F32).astype(BF16)
    arrived = exchange(packed.reshape(experts, capacity, features))

    raw, qdec, ends = local_pass(
        state_probe_logits,
        retention_logits,
        state_source_entries,
        retention_bound_margin,
        extra_fading_amount,
    )
    ends = ends.reshape(members, width // members, 2 * HEAD)
    ends, arrived = lax.optimization_barrier((ends, arrived))
    slices = exchange(ends)

    combined = jnp.zeros((TOK_DEV, features), F32)
    count = capacity // GROUPS
    n = members * count // CHUNKS
    flat_in = arrived.reshape(CHUNKS, -1, features)
    at = jnp.arange(n, dtype=jnp.int32)
    where = at // count * capacity + at % count
    owns = []
    for k in range(GROUPS):
        chosen = (where + k * count)[:, None] == jnp.arange(flat_in.shape[1])[None, :]
        for c in range(CHUNKS):
            owns.append(
                jnp.dot(chosen.astype(BF16), flat_in[c], preferred_element_type=F32).astype(BF16)
            )
    parts = []
    for k in range(GROUPS):
        for c in range(CHUNKS):
            i = k * CHUNKS + c
            own = owns[i]
            if i >= 2:
                own, gate = lax.optimization_barrier((own, parts[i - 2][1]))
                parts[i - 2] = (parts[i - 2][0], gate)
            far = shift(own, 2)
            parts.append(expert_block(own, far, gates, ups, downs))
            if i == 1:
                entering = exchange(prefix_pass(slices)).reshape(width, HEAD)
    rec = output_pass(raw, qdec, entering, state_result_switch_logits, state_result_scale)
    parts[-1], rec = lax.optimization_barrier((parts[-1], rec))
    for k in range(GROUPS):
        first = k * count
        finished = []
        for c in range(CHUNKS):
            mine, other = parts[k * CHUNKS + c]
            back = shift(other, 2)
            finished.append((mine.astype(F32) + back.astype(F32)).astype(BF16))
        finished = jnp.concatenate(finished, axis=0)
        returned = exchange(finished.reshape(members, count, features))
        share = jnp.where(slots_of(first, count), weight[:, None, :], 0.0)
        share = share.reshape(experts * count, TOK_DEV)
        coarse = share.astype(BF16)
        fine = (share - coarse.astype(F32)).astype(BF16)
        flat = returned.reshape(members * count, features)
        if k == GROUPS - 1:
            moe_out = finish(flat, coarse, fine, combined, trailing_scale_vector)
        else:
            for piece in (coarse, fine):
                combined = combined + lax.dot_general(
                    piece, flat, (((0,), (0,)), ((), ())), preferred_element_type=F32
                )

    own, left, right, far = rec, shift(rec, 1), shift(rec, -1), shift(rec, 2)
    by_block = state_result_matrix.reshape(ring, width, -1)

    def columns(block, at):
        held = lax.dynamic_index_in_dim(by_block, lax.rem(place + at, ring), 0, keepdims=False)
        return jnp.dot(block, held, preferred_element_type=F32)

    mixed = columns(own, 0) + columns(left, ring - 1) + columns(right, 1) + columns(far, 2)
    mixer_out = mixed.astype(BF16)
    return (mixer_out, moe_out)


def solution(mesh):
    finer = Mesh(mesh.devices.reshape(8, 4, 2, mesh.shape["tp"]), ("ep_0", "ep_1", "ep_2", "tp"))
    placed = (
        P(EP, "tp"),
        P(EP, "tp"),
        P(EP, "tp"),
        P(EP, "tp"),
        P("tp"),
        P(EP, "tp"),
        P("tp"),
        P(None, "tp"),
        P(EP, None),
        P(EP, None),
        P(EP, None),
        P(),
        P(),
        P(EP, None, "tp"),
        P(EP, None, "tp"),
        P(EP, "tp", None),
    )

    return jax.shard_map(
        shards,
        mesh=finer,
        in_specs=placed,
        out_specs=(P(EP, "tp"), P(EP_TP, None)),
        check_vma=False,
    )
```

```python
import functools

import jax
import jax.numpy as jnp
from jax import lax
from jax.experimental import pallas as pl
from jax.experimental.pallas import tpu as pltpu
from jax.sharding import Mesh
from jax.sharding import PartitionSpec as P

HEAD = 128
SPAN = 128
TOK_DEV = 128
EP = ("ep_0", "ep_1", "ep_2")
EP_TP = ("ep_0", "ep_1", "ep_2", "tp")
GROUPS = 2
CHUNKS = 2


NORM_EPS = 1e-06
SWISH_ALPHA = 1.702
CLAMP_LIMIT = 7.0

F32 = jnp.float32
BF16 = jnp.bfloat16


def rms_scale(values, gain):
    return values * lax.rsqrt(jnp.mean(values * values, axis=-1, keepdims=True) + NORM_EPS) * gain


def log_one_minus(x):
    total = jnp.full_like(x, 1.0 / 9.0)
    for k in range(8, 0, -1):
        total = total * x + 1.0 / k
    return -(x * total)


def split3(x):
    hi = x.astype(BF16)
    rest = x - hi.astype(F32)
    mid = rest.astype(BF16)
    low = (rest - mid.astype(F32)).astype(BF16)
    return hi, mid, low


def local_kernel(q_ref, r_ref, v_ref, m_ref, fade_ref, raw_ref, qdec_ref, st_ref):
    rows, width = q_ref.shape
    heads = width // HEAD
    steps = rows // SPAN
    row = lax.broadcasted_iota(jnp.int32, (SPAN, SPAN), 0)
    col = lax.broadcasted_iota(jnp.int32, (SPAN, SPAN), 1)
    lower = row >= col
    tri = lower.astype(F32).astype(BF16)
    margin = m_ref[...]

    def step(n, carry):
        base, states = carry
        at = pl.ds(pl.multiple_of(n * SPAN, SPAN), SPAN)
        q = q_ref[at, :].astype(F32)
        q = q / (1.0 + jnp.exp(-q)) * HEAD ** (-0.5)
        key = margin / (1.0 + jnp.exp(r_ref[at, :].astype(F32)))
        value = v_ref[at, :]
        fade = fade_ref[at, :]
        fade = jnp.concatenate(
            [jnp.broadcast_to(fade[:, h : h + 1], (SPAN, HEAD)) for h in range(heads)], axis=1
        )
        decay = log_one_minus(key) + fade
        cumul = sum(
            jnp.dot(tri, piece, preferred_element_type=F32) for piece in reversed(split3(decay))
        )
        middle = cumul[SPAN // 2 - 1 : SPAN // 2, :]
        last = cumul[SPAN - 1 : SPAN, :]
        grow = jnp.exp(cumul - middle)
        q_mid = (q * grow).astype(BF16)
        k_mid = (key * jnp.exp(middle - cumul)).astype(BF16)
        q_start = (q * jnp.exp(cumul)).astype(BF16)
        k_end = (key * jnp.exp(last - cumul)).astype(BF16)
        qdec_ref[at, :] = (q * jnp.exp(cumul + base)).astype(BF16)
        block_decay = jnp.exp(last)
        after = []
        for h in range(heads):
            c = slice(h * HEAD, (h + 1) * HEAD)
            scores = lax.dot_general(
                q_mid[:, c], k_mid[:, c], (((1,), (1,)), ((), ())), preferred_element_type=F32
            )
            scores = jnp.where(lower, scores, 0.0).astype(BF16)
            inner = jnp.dot(scores, value[:, c], preferred_element_type=F32)
            outer = jnp.dot(q_start[:, c], states[h].astype(BF16), preferred_element_type=F32)
            raw_ref[at, c] = inner + outer
            update = lax.dot_general(
                k_end[:, c], value[:, c], (((0,), (0,)), ((), ())), preferred_element_type=F32
            )
            wide = jnp.transpose(jnp.broadcast_to(block_decay[:, c], (HEAD, HEAD)))
            after.append(wide * states[h] + update)
        return base + last, tuple(after)

    base, states = lax.fori_loop(
        0,
        steps,
        step,
        (jnp.zeros((1, width), F32), tuple(jnp.zeros((HEAD, HEAD), F32) for _ in range(heads))),
    )
    total = jnp.exp(base)
    for h in range(heads):
        c = slice(h * HEAD, (h + 1) * HEAD)
        st_ref[c, :HEAD] = states[h]
        st_ref[c, HEAD:] = jnp.transpose(jnp.broadcast_to(total[:, c], (HEAD, HEAD)))


def prefix_kernel(x_ref, out_ref):
    state = jnp.zeros(out_ref.shape[1:], F32)
    for i in range(x_ref.shape[0]):
        out_ref[i] = state.astype(BF16)
        state = x_ref[i, :, HEAD:] * state + x_ref[i, :, :HEAD]


def output_kernel(raw_ref, qdec_ref, e_ref, gate_ref, scale_ref, out_ref):
    rows, width = raw_ref.shape
    tile = 256

    def step(n, carry):
        at = pl.ds(pl.multiple_of(n * tile, tile), tile)
        for h in range(width // HEAD):
            c = slice(h * HEAD, (h + 1) * HEAD)
            raw = raw_ref[at, c] + jnp.dot(
                qdec_ref[at, c], e_ref[c, :], preferred_element_type=F32
            )
            normed = raw * lax.rsqrt(jnp.mean(raw * raw, axis=-1, keepdims=True) + NORM_EPS)
            gate = gate_ref[at, c].astype(F32)
            out_ref[at, c] = (
                normed * scale_ref[:, c] * (gate / (1.0 + jnp.exp(-gate)))
            ).astype(BF16)
        return carry

    lax.fori_loop(0, rows // tile, step, 0)


def vmem_call(kernel, outs, flops, bytes_accessed, transcendentals):
    return pl.pallas_call(
        kernel,
        out_shape=outs,
        cost_estimate=pl.CostEstimate(
            flops=flops, bytes_accessed=bytes_accessed, transcendentals=transcendentals
        ),
    )


def local_pass(q, r, v, margin, fade):
    rows, width = q.shape
    return vmem_call(
        local_kernel,
        (
            jax.ShapeDtypeStruct((rows, width), F32),
            jax.ShapeDtypeStruct((rows, width), BF16),
            jax.ShapeDtypeStruct((width, 2 * HEAD), F32),
        ),
        4_000_000_000,
        6 << 20,
        rows * width * 6,
    )(q, r, v, margin.reshape(1, width), fade)


def prefix_pass(x):
    return vmem_call(
        prefix_kernel,
        jax.ShapeDtypeStruct((x.shape[0], x.shape[1], HEAD), BF16),
        100_000_000,
        1 << 19,
        0,
    )(x)


def output_pass(raw, qdec, entering, gate, scale):
    rows, width = raw.shape
    return vmem_call(
        output_kernel,
        jax.ShapeDtypeStruct((rows, width), BF16),
        2_000_000_000,
        4 << 20,
        rows * width * 2,
    )(raw, qdec, entering, gate, scale.reshape(1, width))


def shift(x, by):
    n = lax.axis_size("tp")
    return lax.ppermute(x, "tp", [(i, (i + by) % n) for i in range(n)])


def expert_kernel(
    own,
    far,
    gate_own,
    gate_right,
    gate_left,
    up_own,
    up_right,
    up_left,
    down_own,
    down_right,
    down_left,
    out_own,
    out_far,
    rows,
    gate_w,
    up_w,
    down_w,
    hidden,
    out,
    sems,
    out_sems,
):
    n = own.shape[0]
    tile = gate_right.shape[1]
    wide = 512
    tiles = gate_w.shape[1] // tile

    def columns(owned, right, left):
        return [owned.at[:, pl.ds(0, tile)], owned.at[:, pl.ds(tile, tile)], right, left]

    gates = columns(gate_own, gate_right, gate_left)
    ups = columns(up_own, up_right, up_left)
    downs = [down_own.at[pl.ds(0, tile), :], down_own.at[pl.ds(tile, tile), :]]
    downs += [down_right, down_left]
    places = [pl.ds(f * tile, tile) for f in range(tiles)]
    loads = [
        pltpu.make_async_copy(own, rows.at[pl.ds(0, n), :], sems.at[0]),
        pltpu.make_async_copy(far, rows.at[pl.ds(n, n), :], sems.at[1]),
    ]
    for f in range(tiles):
        loads.append(pltpu.make_async_copy(gates[f], gate_w.at[:, places[f]], sems.at[2 + 2 * f]))
        loads.append(pltpu.make_async_copy(ups[f], up_w.at[:, places[f]], sems.at[3 + 2 * f]))
    for f in range(tiles):
        to = down_w.at[places[f], :]
        loads.append(pltpu.make_async_copy(downs[f], to, sems.at[2 + 2 * tiles + f]))
    for load in loads:
        load.start()
    loads[0].wait()
    loads[1].wait()

    def hidden_tile(f, carry):
        for k in range(tiles):

            @pl.when(f == k)
            def _():
                loads[2 + 2 * k].wait()
                loads[3 + 2 * k].wait()

        at = pl.ds(pl.multiple_of(f * tile, tile), tile)
        gate = jnp.dot(rows[...], gate_w[:, at], preferred_element_type=F32)
        upward = jnp.dot(rows[...], up_w[:, at], preferred_element_type=F32)
        glued = jnp.minimum(gate, CLAMP_LIMIT)
        linear = jnp.clip(upward, -CLAMP_LIMIT, CLAMP_LIMIT)
        act = glued / (1.0 + jnp.exp(-SWISH_ALPHA * glued)) * (linear + 1.0)
        hidden[:, at] = act.astype(BF16)
        return carry

    lax.fori_loop(0, tiles, hidden_tile, 0)
    for load in loads[2 + 2 * tiles :]:
        load.wait()

    stores = []
    for t in range(out.shape[1] // wide):
        at = pl.ds(t * wide, wide)
        stores.append(
            (
                pltpu.make_async_copy(
                    out.at[pl.ds(0, n), at], out_own.at[:, at], out_sems.at[2 * t]
                ),
                pltpu.make_async_copy(
                    out.at[pl.ds(n, n), at], out_far.at[:, at], out_sems.at[2 * t + 1]
                ),
            )
        )

    def out_tile(t, carry):
        at = pl.ds(pl.multiple_of(t * wide, wide), wide)
        part = jnp.dot(hidden[...], down_w[:, at], preferred_element_type=F32)
        out[:, at] = part.astype(BF16)
        for k, pair in enumerate(stores):

            @pl.when(t == k)
            def _():
                for store in pair:
                    store.start()

        return carry

    lax.fori_loop(0, len(stores), out_tile, 0)
    for pair in stores:
        for store in pair:
            store.wait()


def expert_block(own, far, gates, ups, downs):
    n, features = own.shape
    units = sum(w.shape[1] for w in gates)
    hbm = pl.BlockSpec(memory_space=pltpu.HBM)
    return pl.pallas_call(
        expert_kernel,
        out_shape=[jax.ShapeDtypeStruct((n, features), BF16)] * 2,
        in_specs=[hbm] * 11,
        out_specs=[hbm] * 2,
        scratch_shapes=[
            pltpu.VMEM((2 * n, features), BF16),
            pltpu.VMEM((features, units), BF16),
            pltpu.VMEM((features, units), BF16),
            pltpu.VMEM((units, features), BF16),
            pltpu.VMEM((2 * n, units), BF16),
            pltpu.VMEM((2 * n, features), BF16),
            pltpu.SemaphoreType.DMA((14,)),
            pltpu.SemaphoreType.DMA((8,)),
        ],
        cost_estimate=pl.CostEstimate(
            flops=12 * n * features * units,
            bytes_accessed=6 * features * units + 8 * n * features,
            transcendentals=2 * n * units,
        ),
        name="expert_block",
    )(own, far, *gates, *ups, *downs)


def finish_kernel(flat_ref, coarse_ref, fine_ref, partial_ref, gain_ref, out_ref):
    total = partial_ref[...]
    for share in (coarse_ref, fine_ref):
        total = total + lax.dot_general(
            share[...], flat_ref[...], (((0,), (0,)), ((), ())), preferred_element_type=F32
        )
    out_ref[...] = rms_scale(total, gain_ref[...]).astype(BF16)


def finish(flat, coarse, fine, partial, gain):
    tokens, features = partial.shape
    return vmem_call(
        finish_kernel,
        jax.ShapeDtypeStruct((tokens, features), BF16),
        4 * flat.shape[0] * tokens * features,
        4 << 20,
        tokens,
    )(flat, coarse, fine, partial, gain.reshape(1, features))


def halves(weight, dim):
    half = weight.shape[dim] // 2
    return (
        lax.slice_in_dim(weight, 0, half, axis=dim),
        lax.slice_in_dim(weight, half, 2 * half, axis=dim),
    )


def widened(weight, pieces):
    first, second = pieces
    return weight, shift(first, -1), shift(second, 1)


def exchange(x):
    return lax.all_to_all(x, EP, split_axis=0, concat_axis=0, tiled=True)


def shards(
    state_probe_logits,
    retention_logits,
    state_source_entries,
    state_result_switch_logits,
    retention_bound_margin,
    extra_fading_amount,
    state_result_scale,
    state_result_matrix,
    second_slice_tokens,
    specialist_assignment,
    selected_specialist_share,
    leading_scale_vector,
    trailing_scale_vector,
    specialist_switch_matrix,
    specialist_widen_matrix,
    specialist_contract_matrix,
):
    total_rows, width = state_probe_logits.shape
    members = lax.axis_size(EP)
    place = lax.axis_index("tp")
    ring = lax.axis_size("tp")
    features = second_slice_tokens.shape[1]

    own_route = lax.dynamic_slice_in_dim(specialist_assignment, place * TOK_DEV, TOK_DEV, 0)
    own_share = lax.dynamic_slice_in_dim(selected_specialist_share, place * TOK_DEV, TOK_DEV, 0)
    own_rows = lax.dynamic_slice_in_dim(second_slice_tokens, place * TOK_DEV, TOK_DEV, 0)

    down_halves = halves(specialist_contract_matrix[0], 0)
    down_halves, own_rows = lax.optimization_barrier((down_halves, own_rows))
    downs = widened(specialist_contract_matrix[0], down_halves)
    gates = widened(specialist_switch_matrix[0], halves(specialist_switch_matrix[0], 1))
    up_halves = halves(specialist_widen_matrix[0], 1)
    up_halves, retention_logits = lax.optimization_barrier((up_halves, retention_logits))
    ups = widened(specialist_widen_matrix[0], up_halves)
    normed = rms_scale(own_rows.astype(F32), leading_scale_vector).astype(BF16)
    experts = specialist_switch_matrix.shape[0] * members
    capacity = 2 * TOK_DEV * own_route.shape[1] // experts
    expert_ids = jnp.arange(experts, dtype=jnp.int32)[:, None]
    named = [(own_route[:, k][None, :] == expert_ids) for k in range(own_route.shape[1])]
    member = functools.reduce(jnp.logical_or, named)
    weight = sum(jnp.where(named[k], own_share[:, k][None, :], 0.0) for k in range(len(named)))
    ahead = jnp.arange(TOK_DEV)[:, None] < jnp.arange(TOK_DEV)[None, :]
    rank = jnp.dot(
        member.astype(BF16), ahead.astype(BF16), preferred_element_type=F32
    ).astype(jnp.int32)

    def slots_of(first, count):
        ids = first + jnp.arange(count, dtype=jnp.int32)
        return member[:, None, :] & (rank[:, None, :] == ids[None, :, None])

    pick = slots_of(0, capacity).astype(BF16).reshape(experts * capacity, TOK_DEV)
    packed = jnp.dot(pick, normed, preferred_element_type=F32).astype(BF16)
    arrived = exchange(packed.reshape(experts, capacity, features))

    raw, qdec, ends = local_pass(
        state_probe_logits,
        retention_logits,
        state_source_entries,
        retention_bound_margin,
        extra_fading_amount,
    )
    ends = ends.reshape(members, width // members, 2 * HEAD)
    ends, arrived = lax.optimization_barrier((ends, arrived))
    slices = exchange(ends)

    shares = []
    for k in range(GROUPS):
        chosen = slots_of(k * (capacity // GROUPS), capacity // GROUPS)
        share = jnp.where(chosen, weight[:, None, :], 0.0).reshape(-1, TOK_DEV)
        coarse = share.astype(BF16)
        fine = (share - coarse.astype(F32)).astype(BF16)
        shares.append((coarse, fine))

    combined = jnp.zeros((TOK_DEV, features), F32)
    count = capacity // GROUPS
    n = members * count // CHUNKS
    flat_in = arrived.reshape(CHUNKS, -1, features)
    at = jnp.arange(n, dtype=jnp.int32)
    where = at // count * capacity + at % count
    owns = []
    for k in range(GROUPS):
        chosen = (where + k * count)[:, None] == jnp.arange(flat_in.shape[1])[None, :]
        for c in range(CHUNKS):
            owns.append(
                jnp.dot(chosen.astype(BF16), flat_in[c], preferred_element_type=F32).astype(BF16)
            )
    parts = []
    for k in range(GROUPS):
        for c in range(CHUNKS):
            i = k * CHUNKS + c
            own = owns[i]
            far = shift(own, 2)
            parts.append(expert_block(own, far, gates, ups, downs))
            if i == 1:
                leaving = prefix_pass(slices)
    for k in range(GROUPS):
        finished = []
        for c in range(CHUNKS):
            mine, other = parts[k * CHUNKS + c]
            back = shift(other, 2)
            total = (mine.astype(F32) + back.astype(F32)).astype(BF16)
            if k == 0:
                beside = leaving.reshape(CHUNKS, n, HEAD)[c]
                total = jnp.concatenate([total, beside], axis=1)
            finished.append(total)
        finished = jnp.concatenate(finished, axis=0).reshape(members, count, -1)
        returned = exchange(finished)
        if k == 0:
            entering = returned[:, :, features:].reshape(width, HEAD)
            returned = returned[:, :, :features]
            rec = output_pass(raw, qdec, entering, state_result_switch_logits, state_result_scale)
        coarse, fine = shares[k]
        flat = returned.reshape(members * count, features)
        if k == GROUPS - 1:
            moe_out = finish(flat, coarse, fine, combined, trailing_scale_vector)
        else:
            for piece in (coarse, fine):
                combined = combined + lax.dot_general(
                    piece, flat, (((0,), (0,)), ((), ())), preferred_element_type=F32
                )

    half = total_rows // 2
    own, left, right = rec, shift(rec, 1), shift(rec, -1)
    far = jnp.concatenate([shift(left[:half], 1), shift(right[half:], -1)], axis=0)
    by_block = state_result_matrix.reshape(ring, width, -1)

    def columns(block, at):
        held = lax.dynamic_index_in_dim(by_block, lax.rem(place + at, ring), 0, keepdims=False)
        return jnp.dot(block, held, preferred_element_type=F32)

    mixed = columns(own, 0) + columns(left, ring - 1) + columns(right, 1) + columns(far, 2)
    mixer_out = mixed.astype(BF16)
    return (mixer_out, moe_out)


def solution(mesh):
    finer = Mesh(mesh.devices.reshape(8, 4, 2, mesh.shape["tp"]), ("ep_0", "ep_1", "ep_2", "tp"))
    placed = (
        P(EP, "tp"),
        P(EP, "tp"),
        P(EP, "tp"),
        P(EP, "tp"),
        P("tp"),
        P(EP, "tp"),
        P("tp"),
        P(None, "tp"),
        P(EP, None),
        P(EP, None),
        P(EP, None),
        P(),
        P(),
        P(EP, None, "tp"),
        P(EP, None, "tp"),
        P(EP, "tp", None),
    )

    return jax.shard_map(
        shards,
        mesh=finer,
        in_specs=placed,
        out_specs=(P(EP, "tp"), P(EP_TP, None)),
        check_vma=False,
    )
```

```python
import functools

import jax
import jax.numpy as jnp
from jax import lax
from jax.experimental import pallas as pl
from jax.experimental.pallas import tpu as pltpu
from jax.sharding import Mesh
from jax.sharding import PartitionSpec as P

HEAD = 128
SPAN = 128
TOK_DEV = 128
EP = ("ep_0", "ep_1", "ep_2")
EP_TP = ("ep_0", "ep_1", "ep_2", "tp")
GROUPS = 2
CHUNKS = 2


NORM_EPS = 1e-06
SWISH_ALPHA = 1.702
CLAMP_LIMIT = 7.0

F32 = jnp.float32
BF16 = jnp.bfloat16


def rms_scale(values, gain):
    return values * lax.rsqrt(jnp.mean(values * values, axis=-1, keepdims=True) + NORM_EPS) * gain


def log_one_minus(x):
    total = jnp.full_like(x, 1.0 / 9.0)
    for k in range(8, 0, -1):
        total = total * x + 1.0 / k
    return -(x * total)


def split3(x):
    hi = x.astype(BF16)
    rest = x - hi.astype(F32)
    mid = rest.astype(BF16)
    low = (rest - mid.astype(F32)).astype(BF16)
    return hi, mid, low


def local_kernel(q_ref, r_ref, v_ref, m_ref, fade_ref, raw_ref, qdec_ref, st_ref):
    rows, width = q_ref.shape
    heads = width // HEAD
    steps = rows // SPAN
    row = lax.broadcasted_iota(jnp.int32, (SPAN, SPAN), 0)
    col = lax.broadcasted_iota(jnp.int32, (SPAN, SPAN), 1)
    lower = row >= col
    tri = lower.astype(F32).astype(BF16)
    margin = m_ref[...]

    def step(n, carry):
        base, states = carry
        at = pl.ds(pl.multiple_of(n * SPAN, SPAN), SPAN)
        q = q_ref[at, :].astype(F32)
        q = q / (1.0 + jnp.exp(-q)) * HEAD ** (-0.5)
        key = margin / (1.0 + jnp.exp(r_ref[at, :].astype(F32)))
        value = v_ref[at, :]
        fade = fade_ref[at, :]
        fade = jnp.concatenate(
            [jnp.broadcast_to(fade[:, h : h + 1], (SPAN, HEAD)) for h in range(heads)], axis=1
        )
        decay = log_one_minus(key) + fade
        cumul = sum(
            jnp.dot(tri, piece, preferred_element_type=F32) for piece in reversed(split3(decay))
        )
        middle = cumul[SPAN // 2 - 1 : SPAN // 2, :]
        last = cumul[SPAN - 1 : SPAN, :]
        grow = jnp.exp(cumul - middle)
        q_mid = (q * grow).astype(BF16)
        k_mid = (key * jnp.exp(middle - cumul)).astype(BF16)
        q_start = (q * jnp.exp(cumul)).astype(BF16)
        k_end = (key * jnp.exp(last - cumul)).astype(BF16)
        qdec_ref[at, :] = (q * jnp.exp(cumul + base)).astype(BF16)
        block_decay = jnp.exp(last)
        after = []
        for h in range(heads):
            c = slice(h * HEAD, (h + 1) * HEAD)
            scores = lax.dot_general(
                q_mid[:, c], k_mid[:, c], (((1,), (1,)), ((), ())), preferred_element_type=F32
            )
            scores = jnp.where(lower, scores, 0.0).astype(BF16)
            inner = jnp.dot(scores, value[:, c], preferred_element_type=F32)
            outer = jnp.dot(q_start[:, c], states[h].astype(BF16), preferred_element_type=F32)
            raw_ref[at, c] = inner + outer
            update = lax.dot_general(
                k_end[:, c], value[:, c], (((0,), (0,)), ((), ())), preferred_element_type=F32
            )
            wide = jnp.transpose(jnp.broadcast_to(block_decay[:, c], (HEAD, HEAD)))
            after.append(wide * states[h] + update)
        return base + last, tuple(after)

    base, states = lax.fori_loop(
        0,
        steps,
        step,
        (jnp.zeros((1, width), F32), tuple(jnp.zeros((HEAD, HEAD), F32) for _ in range(heads))),
    )
    total = jnp.exp(base)
    for h in range(heads):
        c = slice(h * HEAD, (h + 1) * HEAD)
        st_ref[c, :HEAD] = states[h]
        st_ref[c, HEAD:] = jnp.transpose(jnp.broadcast_to(total[:, c], (HEAD, HEAD)))


def prefix_kernel(x_ref, out_ref):
    state = jnp.zeros(out_ref.shape[1:], F32)
    for i in range(x_ref.shape[0]):
        out_ref[i] = state.astype(BF16)
        state = x_ref[i, :, HEAD:] * state + x_ref[i, :, :HEAD]


def output_kernel(raw_ref, qdec_ref, e_ref, gate_ref, scale_ref, out_ref):
    rows, width = raw_ref.shape
    tile = 256

    def step(n, carry):
        at = pl.ds(pl.multiple_of(n * tile, tile), tile)
        for h in range(width // HEAD):
            c = slice(h * HEAD, (h + 1) * HEAD)
            raw = raw_ref[at, c] + jnp.dot(
                qdec_ref[at, c], e_ref[c, :], preferred_element_type=F32
            )
            normed = raw * lax.rsqrt(jnp.mean(raw * raw, axis=-1, keepdims=True) + NORM_EPS)
            gate = gate_ref[at, c].astype(F32)
            out_ref[at, c] = (
                normed * scale_ref[:, c] * (gate / (1.0 + jnp.exp(-gate)))
            ).astype(BF16)
        return carry

    lax.fori_loop(0, rows // tile, step, 0)


def vmem_call(kernel, outs, flops, bytes_accessed, transcendentals):
    return pl.pallas_call(
        kernel,
        out_shape=outs,
        cost_estimate=pl.CostEstimate(
            flops=flops, bytes_accessed=bytes_accessed, transcendentals=transcendentals
        ),
    )


def local_pass(q, r, v, margin, fade):
    rows, width = q.shape
    return vmem_call(
        local_kernel,
        (
            jax.ShapeDtypeStruct((rows, width), F32),
            jax.ShapeDtypeStruct((rows, width), BF16),
            jax.ShapeDtypeStruct((width, 2 * HEAD), F32),
        ),
        4_000_000_000,
        6 << 20,
        rows * width * 6,
    )(q, r, v, margin.reshape(1, width), fade)


def prefix_pass(x):
    return vmem_call(
        prefix_kernel,
        jax.ShapeDtypeStruct((x.shape[0], x.shape[1], HEAD), BF16),
        100_000_000,
        1 << 19,
        0,
    )(x)


def output_pass(raw, qdec, entering, gate, scale):
    rows, width = raw.shape
    return vmem_call(
        output_kernel,
        jax.ShapeDtypeStruct((rows, width), BF16),
        2_000_000_000,
        4 << 20,
        rows * width * 2,
    )(raw, qdec, entering, gate, scale.reshape(1, width))


def shift(x, by):
    n = lax.axis_size("tp")
    return lax.ppermute(x, "tp", [(i, (i + by) % n) for i in range(n)])


def expert_kernel(
    own,
    far,
    gate_own,
    gate_right,
    gate_left,
    up_own,
    up_right,
    up_left,
    down_own,
    down_right,
    down_left,
    out_own,
    out_far,
    rows,
    gate_w,
    up_w,
    down_w,
    hidden,
    out,
    sems,
    out_sems,
):
    n = own.shape[0]
    tile = gate_right.shape[1]
    wide = 512
    tiles = gate_w.shape[1] // tile

    def columns(owned, right, left):
        return [owned.at[:, pl.ds(0, tile)], owned.at[:, pl.ds(tile, tile)], right, left]

    gates = columns(gate_own, gate_right, gate_left)
    ups = columns(up_own, up_right, up_left)
    downs = [down_own.at[pl.ds(0, tile), :], down_own.at[pl.ds(tile, tile), :]]
    downs += [down_right, down_left]
    places = [pl.ds(f * tile, tile) for f in range(tiles)]
    loads = [
        pltpu.make_async_copy(own, rows.at[pl.ds(0, n), :], sems.at[0]),
        pltpu.make_async_copy(far, rows.at[pl.ds(n, n), :], sems.at[1]),
    ]
    for f in range(tiles):
        loads.append(pltpu.make_async_copy(gates[f], gate_w.at[:, places[f]], sems.at[2 + 2 * f]))
        loads.append(pltpu.make_async_copy(ups[f], up_w.at[:, places[f]], sems.at[3 + 2 * f]))
    for f in range(tiles):
        to = down_w.at[places[f], :]
        loads.append(pltpu.make_async_copy(downs[f], to, sems.at[2 + 2 * tiles + f]))
    batches = [loads[:4], loads[4:6]]
    batches += [loads[2 + 2 * f : 4 + 2 * f] for f in range(2, tiles)]
    batches += [loads[2 + 2 * tiles : 4 + 2 * tiles], loads[4 + 2 * tiles :]]
    for load in batches[0] + batches[1]:
        load.start()

    def hidden_tile(f, carry):
        for k in range(tiles):

            @pl.when(f == k)
            def _():
                for load in batches[k]:
                    load.wait()
                for load in batches[k + 2]:
                    load.start()

        at = pl.ds(pl.multiple_of(f * tile, tile), tile)
        gate = jnp.dot(rows[...], gate_w[:, at], preferred_element_type=F32)
        upward = jnp.dot(rows[...], up_w[:, at], preferred_element_type=F32)
        glued = jnp.minimum(gate, CLAMP_LIMIT)
        linear = jnp.clip(upward, -CLAMP_LIMIT, CLAMP_LIMIT)
        act = glued / (1.0 + jnp.exp(-SWISH_ALPHA * glued)) * (linear + 1.0)
        hidden[:, at] = act.astype(BF16)
        return carry

    lax.fori_loop(0, tiles, hidden_tile, 0)
    for load in loads[2 + 2 * tiles :]:
        load.wait()

    stores = []
    for t in range(out.shape[1] // wide):
        at = pl.ds(t * wide, wide)
        stores.append(
            (
                pltpu.make_async_copy(
                    out.at[pl.ds(0, n), at], out_own.at[:, at], out_sems.at[2 * t]
                ),
                pltpu.make_async_copy(
                    out.at[pl.ds(n, n), at], out_far.at[:, at], out_sems.at[2 * t + 1]
                ),
            )
        )

    def out_tile(t, carry):
        at = pl.ds(pl.multiple_of(t * wide, wide), wide)
        part = jnp.dot(hidden[...], down_w[:, at], preferred_element_type=F32)
        out[:, at] = part.astype(BF16)
        for k, pair in enumerate(stores):

            @pl.when(t == k)
            def _():
                for store in pair:
                    store.start()

        return carry

    lax.fori_loop(0, len(stores), out_tile, 0)
    for pair in stores:
        for store in pair:
            store.wait()


def expert_block(own, far, gates, ups, downs):
    n, features = own.shape
    units = sum(w.shape[1] for w in gates)
    hbm = pl.BlockSpec(memory_space=pltpu.HBM)
    return pl.pallas_call(
        expert_kernel,
        out_shape=[jax.ShapeDtypeStruct((n, features), BF16)] * 2,
        in_specs=[hbm] * 11,
        out_specs=[hbm] * 2,
        scratch_shapes=[
            pltpu.VMEM((2 * n, features), BF16),
            pltpu.VMEM((features, units), BF16),
            pltpu.VMEM((features, units), BF16),
            pltpu.VMEM((units, features), BF16),
            pltpu.VMEM((2 * n, units), BF16),
            pltpu.VMEM((2 * n, features), BF16),
            pltpu.SemaphoreType.DMA((14,)),
            pltpu.SemaphoreType.DMA((8,)),
        ],
        cost_estimate=pl.CostEstimate(
            flops=12 * n * features * units,
            bytes_accessed=6 * features * units + 8 * n * features,
            transcendentals=2 * n * units,
        ),
        name="expert_block",
    )(own, far, *gates, *ups, *downs)


def finish_kernel(flat_ref, coarse_ref, fine_ref, partial_ref, gain_ref, out_ref):
    total = partial_ref[...]
    for share in (coarse_ref, fine_ref):
        total = total + lax.dot_general(
            share[...], flat_ref[...], (((0,), (0,)), ((), ())), preferred_element_type=F32
        )
    out_ref[...] = rms_scale(total, gain_ref[...]).astype(BF16)


def finish(flat, coarse, fine, partial, gain):
    tokens, features = partial.shape
    return vmem_call(
        finish_kernel,
        jax.ShapeDtypeStruct((tokens, features), BF16),
        4 * flat.shape[0] * tokens * features,
        4 << 20,
        tokens,
    )(flat, coarse, fine, partial, gain.reshape(1, features))


def halves(weight, dim):
    half = weight.shape[dim] // 2
    return (
        lax.slice_in_dim(weight, 0, half, axis=dim),
        lax.slice_in_dim(weight, half, 2 * half, axis=dim),
    )


def widened(weight, pieces):
    first, second = pieces
    return weight, shift(first, -1), shift(second, 1)


def exchange(x):
    return lax.all_to_all(x, EP, split_axis=0, concat_axis=0, tiled=True)


def shards(
    state_probe_logits,
    retention_logits,
    state_source_entries,
    state_result_switch_logits,
    retention_bound_margin,
    extra_fading_amount,
    state_result_scale,
    state_result_matrix,
    second_slice_tokens,
    specialist_assignment,
    selected_specialist_share,
    leading_scale_vector,
    trailing_scale_vector,
    specialist_switch_matrix,
    specialist_widen_matrix,
    specialist_contract_matrix,
):
    total_rows, width = state_probe_logits.shape
    members = lax.axis_size(EP)
    place = lax.axis_index("tp")
    ring = lax.axis_size("tp")
    features = second_slice_tokens.shape[1]

    own_route = lax.dynamic_slice_in_dim(specialist_assignment, place * TOK_DEV, TOK_DEV, 0)
    own_share = lax.dynamic_slice_in_dim(selected_specialist_share, place * TOK_DEV, TOK_DEV, 0)
    own_rows = lax.dynamic_slice_in_dim(second_slice_tokens, place * TOK_DEV, TOK_DEV, 0)

    down_halves = halves(specialist_contract_matrix[0], 0)
    down_halves, own_rows = lax.optimization_barrier((down_halves, own_rows))
    downs = widened(specialist_contract_matrix[0], down_halves)
    gates = widened(specialist_switch_matrix[0], halves(specialist_switch_matrix[0], 1))
    up_halves = halves(specialist_widen_matrix[0], 1)
    up_halves, retention_logits = lax.optimization_barrier((up_halves, retention_logits))
    ups = widened(specialist_widen_matrix[0], up_halves)
    normed = rms_scale(own_rows.astype(F32), leading_scale_vector).astype(BF16)
    experts = specialist_switch_matrix.shape[0] * members
    capacity = 2 * TOK_DEV * own_route.shape[1] // experts
    expert_ids = jnp.arange(experts, dtype=jnp.int32)[:, None]
    named = [(own_route[:, k][None, :] == expert_ids) for k in range(own_route.shape[1])]
    member = functools.reduce(jnp.logical_or, named)
    weight = sum(jnp.where(named[k], own_share[:, k][None, :], 0.0) for k in range(len(named)))
    ahead = jnp.arange(TOK_DEV)[:, None] < jnp.arange(TOK_DEV)[None, :]
    rank = jnp.dot(
        member.astype(BF16), ahead.astype(BF16), preferred_element_type=F32
    ).astype(jnp.int32)

    def slots_of(first, count):
        ids = first + jnp.arange(count, dtype=jnp.int32)
        return member[:, None, :] & (rank[:, None, :] == ids[None, :, None])

    pick = slots_of(0, capacity).astype(BF16).reshape(experts * capacity, TOK_DEV)
    packed = jnp.dot(pick, normed, preferred_element_type=F32).astype(BF16)
    arrived = exchange(packed.reshape(experts, capacity, features))

    raw, qdec, ends = local_pass(
        state_probe_logits,
        retention_logits,
        state_source_entries,
        retention_bound_margin,
        extra_fading_amount,
    )
    ends = ends.reshape(members, width // members, 2 * HEAD)
    ends, arrived = lax.optimization_barrier((ends, arrived))
    slices = exchange(ends)

    shares = []
    for k in range(GROUPS):
        chosen = slots_of(k * (capacity // GROUPS), capacity // GROUPS)
        share = jnp.where(chosen, weight[:, None, :], 0.0).reshape(-1, TOK_DEV)
        coarse = share.astype(BF16)
        fine = (share - coarse.astype(F32)).astype(BF16)
        shares.append((coarse, fine))

    combined = jnp.zeros((TOK_DEV, features), F32)
    count = capacity // GROUPS
    n = members * count // CHUNKS
    flat_in = arrived.reshape(CHUNKS, -1, features)
    at = jnp.arange(n, dtype=jnp.int32)
    where = at // count * capacity + at % count
    owns = []
    for k in range(GROUPS):
        chosen = (where + k * count)[:, None] == jnp.arange(flat_in.shape[1])[None, :]
        for c in range(CHUNKS):
            owns.append(
                jnp.dot(chosen.astype(BF16), flat_in[c], preferred_element_type=F32).astype(BF16)
            )
    parts = []
    for k in range(GROUPS):
        for c in range(CHUNKS):
            i = k * CHUNKS + c
            own = owns[i]
            far = shift(own, 2)
            parts.append(expert_block(own, far, gates, ups, downs))
            if i == 1:
                leaving = prefix_pass(slices)
    for k in range(GROUPS):
        finished = []
        for c in range(CHUNKS):
            mine, other = parts[k * CHUNKS + c]
            back = shift(other, 2)
            total = (mine.astype(F32) + back.astype(F32)).astype(BF16)
            if k == 0:
                beside = leaving.reshape(CHUNKS, n, HEAD)[c]
                total = jnp.concatenate([total, beside], axis=1)
            finished.append(total)
        finished = jnp.concatenate(finished, axis=0).reshape(members, count, -1)
        returned = exchange(finished)
        if k == 0:
            entering = returned[:, :, features:].reshape(width, HEAD)
            returned = returned[:, :, :features]
            rec = output_pass(raw, qdec, entering, state_result_switch_logits, state_result_scale)
        coarse, fine = shares[k]
        flat = returned.reshape(members * count, features)
        if k == GROUPS - 1:
            moe_out = finish(flat, coarse, fine, combined, trailing_scale_vector)
        else:
            for piece in (coarse, fine):
                combined = combined + lax.dot_general(
                    piece, flat, (((0,), (0,)), ((), ())), preferred_element_type=F32
                )

    half = total_rows // 2
    own, left, right = rec, shift(rec, 1), shift(rec, -1)
    far = jnp.concatenate([shift(left[:half], 1), shift(right[half:], -1)], axis=0)
    by_block = state_result_matrix.reshape(ring, width, -1)

    def columns(block, at):
        held = lax.dynamic_index_in_dim(by_block, lax.rem(place + at, ring), 0, keepdims=False)
        return jnp.dot(block, held, preferred_element_type=F32)

    mixed = columns(own, 0) + columns(left, ring - 1) + columns(right, 1) + columns(far, 2)
    mixer_out = mixed.astype(BF16)
    return (mixer_out, moe_out)


def solution(mesh):
    finer = Mesh(mesh.devices.reshape(8, 4, 2, mesh.shape["tp"]), ("ep_0", "ep_1", "ep_2", "tp"))
    placed = (
        P(EP, "tp"),
        P(EP, "tp"),
        P(EP, "tp"),
        P(EP, "tp"),
        P("tp"),
        P(EP, "tp"),
        P("tp"),
        P(None, "tp"),
        P(EP, None),
        P(EP, None),
        P(EP, None),
        P(),
        P(),
        P(EP, None, "tp"),
        P(EP, None, "tp"),
        P(EP, "tp", None),
    )

    return jax.shard_map(
        shards,
        mesh=finer,
        in_specs=placed,
        out_specs=(P(EP, "tp"), P(EP_TP, None)),
        check_vma=False,
    )
```

```python
import functools

import jax
import jax.numpy as jnp
from jax import lax
from jax.experimental import pallas as pl
from jax.experimental.pallas import tpu as pltpu
from jax.sharding import Mesh
from jax.sharding import PartitionSpec as P

HEAD = 128
SPAN = 128
TOK_DEV = 128
EP = ("ep_0", "ep_1", "ep_2")
EP_TP = ("ep_0", "ep_1", "ep_2", "tp")
GROUPS = 2
CHUNKS = 2


NORM_EPS = 1e-06
SWISH_ALPHA = 1.702
CLAMP_LIMIT = 7.0

F32 = jnp.float32
BF16 = jnp.bfloat16


def rms_scale(values, gain):
    return values * lax.rsqrt(jnp.mean(values * values, axis=-1, keepdims=True) + NORM_EPS) * gain


def log_one_minus(x):
    total = jnp.full_like(x, 1.0 / 9.0)
    for k in range(8, 0, -1):
        total = total * x + 1.0 / k
    return -(x * total)


def split3(x):
    hi = x.astype(BF16)
    rest = x - hi.astype(F32)
    mid = rest.astype(BF16)
    low = (rest - mid.astype(F32)).astype(BF16)
    return hi, mid, low


def local_kernel(q_ref, r_ref, v_ref, m_ref, fade_ref, raw_ref, qdec_ref, st_ref):
    rows, width = q_ref.shape
    heads = width // HEAD
    steps = rows // SPAN
    row = lax.broadcasted_iota(jnp.int32, (SPAN, SPAN), 0)
    col = lax.broadcasted_iota(jnp.int32, (SPAN, SPAN), 1)
    lower = row >= col
    tri = lower.astype(F32).astype(BF16)
    margin = m_ref[...]

    def step(n, carry):
        base, states = carry
        at = pl.ds(pl.multiple_of(n * SPAN, SPAN), SPAN)
        q = q_ref[at, :].astype(F32)
        q = q / (1.0 + jnp.exp(-q)) * HEAD ** (-0.5)
        key = margin / (1.0 + jnp.exp(r_ref[at, :].astype(F32)))
        value = v_ref[at, :]
        fade = fade_ref[at, :]
        fade = jnp.concatenate(
            [jnp.broadcast_to(fade[:, h : h + 1], (SPAN, HEAD)) for h in range(heads)], axis=1
        )
        decay = log_one_minus(key) + fade
        cumul = sum(
            jnp.dot(tri, piece, preferred_element_type=F32) for piece in reversed(split3(decay))
        )
        middle = cumul[SPAN // 2 - 1 : SPAN // 2, :]
        last = cumul[SPAN - 1 : SPAN, :]
        grow = jnp.exp(cumul - middle)
        q_mid = (q * grow).astype(BF16)
        k_mid = (key * jnp.exp(middle - cumul)).astype(BF16)
        q_start = (q * jnp.exp(cumul)).astype(BF16)
        k_end = (key * jnp.exp(last - cumul)).astype(BF16)
        qdec_ref[at, :] = (q * jnp.exp(cumul + base)).astype(BF16)
        block_decay = jnp.exp(last)
        after = []
        for h in range(heads):
            c = slice(h * HEAD, (h + 1) * HEAD)
            scores = lax.dot_general(
                q_mid[:, c], k_mid[:, c], (((1,), (1,)), ((), ())), preferred_element_type=F32
            )
            scores = jnp.where(lower, scores, 0.0).astype(BF16)
            inner = jnp.dot(scores, value[:, c], preferred_element_type=F32)
            outer = jnp.dot(q_start[:, c], states[h].astype(BF16), preferred_element_type=F32)
            raw_ref[at, c] = inner + outer
            update = lax.dot_general(
                k_end[:, c], value[:, c], (((0,), (0,)), ((), ())), preferred_element_type=F32
            )
            wide = jnp.transpose(jnp.broadcast_to(block_decay[:, c], (HEAD, HEAD)))
            after.append(wide * states[h] + update)
        return base + last, tuple(after)

    base, states = lax.fori_loop(
        0,
        steps,
        step,
        (jnp.zeros((1, width), F32), tuple(jnp.zeros((HEAD, HEAD), F32) for _ in range(heads))),
    )
    total = jnp.exp(base)
    for h in range(heads):
        c = slice(h * HEAD, (h + 1) * HEAD)
        st_ref[c, :HEAD] = states[h]
        st_ref[c, HEAD:] = jnp.transpose(jnp.broadcast_to(total[:, c], (HEAD, HEAD)))


def prefix_kernel(x_ref, out_ref):
    state = jnp.zeros(out_ref.shape[1:], F32)
    for i in range(x_ref.shape[0]):
        out_ref[i] = state.astype(BF16)
        state = x_ref[i, :, HEAD:] * state + x_ref[i, :, :HEAD]


def output_kernel(raw_ref, qdec_ref, e_ref, gate_ref, scale_ref, out_ref):
    rows, width = raw_ref.shape
    tile = 256

    def step(n, carry):
        at = pl.ds(pl.multiple_of(n * tile, tile), tile)
        for h in range(width // HEAD):
            c = slice(h * HEAD, (h + 1) * HEAD)
            raw = raw_ref[at, c] + jnp.dot(
                qdec_ref[at, c], e_ref[c, :], preferred_element_type=F32
            )
            normed = raw * lax.rsqrt(jnp.mean(raw * raw, axis=-1, keepdims=True) + NORM_EPS)
            gate = gate_ref[at, c].astype(F32)
            out_ref[at, c] = (
                normed * scale_ref[:, c] * (gate / (1.0 + jnp.exp(-gate)))
            ).astype(BF16)
        return carry

    lax.fori_loop(0, rows // tile, step, 0)


def vmem_call(kernel, outs, flops, bytes_accessed, transcendentals):
    return pl.pallas_call(
        kernel,
        out_shape=outs,
        cost_estimate=pl.CostEstimate(
            flops=flops, bytes_accessed=bytes_accessed, transcendentals=transcendentals
        ),
    )


def local_pass(q, r, v, margin, fade):
    rows, width = q.shape
    return vmem_call(
        local_kernel,
        (
            jax.ShapeDtypeStruct((rows, width), F32),
            jax.ShapeDtypeStruct((rows, width), BF16),
            jax.ShapeDtypeStruct((width, 2 * HEAD), F32),
        ),
        4_000_000_000,
        6 << 20,
        rows * width * 6,
    )(q, r, v, margin.reshape(1, width), fade)


def prefix_pass(x):
    return vmem_call(
        prefix_kernel,
        jax.ShapeDtypeStruct((x.shape[0], x.shape[1], HEAD), BF16),
        100_000_000,
        1 << 19,
        0,
    )(x)


def output_pass(raw, qdec, entering, gate, scale):
    rows, width = raw.shape
    return vmem_call(
        output_kernel,
        jax.ShapeDtypeStruct((rows, width), BF16),
        2_000_000_000,
        4 << 20,
        rows * width * 2,
    )(raw, qdec, entering, gate, scale.reshape(1, width))


def shift(x, by):
    n = lax.axis_size("tp")
    return lax.ppermute(x, "tp", [(i, (i + by) % n) for i in range(n)])


def expert_kernel(
    own,
    far,
    gate_own,
    gate_right,
    gate_left,
    up_own,
    up_right,
    up_left,
    down_own,
    down_right,
    down_left,
    out_own,
    out_far,
    rows,
    gate_w,
    up_w,
    down_w,
    hidden,
    out,
    sems,
    out_sems,
):
    n = own.shape[0]
    tile = gate_right.shape[1]
    wide = 512
    tiles = gate_w.shape[1] // tile

    def columns(owned, right, left):
        return [owned.at[:, pl.ds(0, tile)], owned.at[:, pl.ds(tile, tile)], right, left]

    gates = columns(gate_own, gate_right, gate_left)
    ups = columns(up_own, up_right, up_left)
    downs = [down_own.at[pl.ds(0, tile), :], down_own.at[pl.ds(tile, tile), :]]
    downs += [down_right, down_left]
    places = [pl.ds(f * tile, tile) for f in range(tiles)]
    loads = [
        pltpu.make_async_copy(own, rows.at[pl.ds(0, n), :], sems.at[0]),
        pltpu.make_async_copy(far, rows.at[pl.ds(n, n), :], sems.at[1]),
    ]
    for f in range(tiles):
        loads.append(pltpu.make_async_copy(gates[f], gate_w.at[:, places[f]], sems.at[2 + 2 * f]))
        loads.append(pltpu.make_async_copy(ups[f], up_w.at[:, places[f]], sems.at[3 + 2 * f]))
    for f in range(tiles):
        to = down_w.at[places[f], :]
        loads.append(pltpu.make_async_copy(downs[f], to, sems.at[2 + 2 * tiles + f]))
    for load in loads:
        load.start()
    loads[0].wait()
    loads[1].wait()

    def hidden_tile(f, carry):
        for k in range(tiles):

            @pl.when(f == k)
            def _():
                loads[2 + 2 * k].wait()
                loads[3 + 2 * k].wait()

        at = pl.ds(pl.multiple_of(f * tile, tile), tile)
        gate = jnp.dot(rows[...], gate_w[:, at], preferred_element_type=F32)
        upward = jnp.dot(rows[...], up_w[:, at], preferred_element_type=F32)
        glued = jnp.minimum(gate, CLAMP_LIMIT)
        linear = jnp.clip(upward, -CLAMP_LIMIT, CLAMP_LIMIT)
        act = glued / (1.0 + jnp.exp(-SWISH_ALPHA * glued)) * (linear + 1.0)
        hidden[:, at] = act.astype(BF16)
        return carry

    lax.fori_loop(0, tiles, hidden_tile, 0)
    for load in loads[2 + 2 * tiles :]:
        load.wait()

    stores = []
    for t in range(out.shape[1] // wide):
        at = pl.ds(t * wide, wide)
        stores.append(
            (
                pltpu.make_async_copy(
                    out.at[pl.ds(0, n), at], out_own.at[:, at], out_sems.at[2 * t]
                ),
                pltpu.make_async_copy(
                    out.at[pl.ds(n, n), at], out_far.at[:, at], out_sems.at[2 * t + 1]
                ),
            )
        )

    def out_tile(t, carry):
        at = pl.ds(pl.multiple_of(t * wide, wide), wide)
        part = jnp.dot(hidden[...], down_w[:, at], preferred_element_type=F32)
        out[:, at] = part.astype(BF16)
        for k, pair in enumerate(stores):

            @pl.when(t == k)
            def _():
                for store in pair:
                    store.start()

        return carry

    lax.fori_loop(0, len(stores), out_tile, 0)
    for pair in stores:
        for store in pair:
            store.wait()


def expert_block(own, far, gates, ups, downs):
    n, features = own.shape
    units = sum(w.shape[1] for w in gates)
    hbm = pl.BlockSpec(memory_space=pltpu.HBM)
    return pl.pallas_call(
        expert_kernel,
        out_shape=[jax.ShapeDtypeStruct((n, features), BF16)] * 2,
        in_specs=[hbm] * 11,
        out_specs=[hbm] * 2,
        scratch_shapes=[
            pltpu.VMEM((2 * n, features), BF16),
            pltpu.VMEM((features, units), BF16),
            pltpu.VMEM((features, units), BF16),
            pltpu.VMEM((units, features), BF16),
            pltpu.VMEM((2 * n, units), BF16),
            pltpu.VMEM((2 * n, features), BF16),
            pltpu.SemaphoreType.DMA((14,)),
            pltpu.SemaphoreType.DMA((8,)),
        ],
        cost_estimate=pl.CostEstimate(
            flops=12 * n * features * units,
            bytes_accessed=6 * features * units + 8 * n * features,
            transcendentals=2 * n * units,
        ),
        name="expert_block",
    )(own, far, *gates, *ups, *downs)


def finish_kernel(flat_ref, coarse_ref, fine_ref, partial_ref, gain_ref, out_ref):
    total = partial_ref[...]
    for share in (coarse_ref, fine_ref):
        total = total + lax.dot_general(
            share[...], flat_ref[...], (((0,), (0,)), ((), ())), preferred_element_type=F32
        )
    out_ref[...] = rms_scale(total, gain_ref[...]).astype(BF16)


def finish(flat, coarse, fine, partial, gain):
    tokens, features = partial.shape
    return vmem_call(
        finish_kernel,
        jax.ShapeDtypeStruct((tokens, features), BF16),
        4 * flat.shape[0] * tokens * features,
        4 << 20,
        tokens,
    )(flat, coarse, fine, partial, gain.reshape(1, features))


def halves(weight, dim):
    half = weight.shape[dim] // 2
    return (
        lax.slice_in_dim(weight, 0, half, axis=dim),
        lax.slice_in_dim(weight, half, 2 * half, axis=dim),
    )


def widened(weight, pieces):
    first, second = pieces
    return weight, shift(first, -1), shift(second, 1)


def exchange(x):
    return lax.all_to_all(x, EP, split_axis=0, concat_axis=0, tiled=True)


def shards(
    state_probe_logits,
    retention_logits,
    state_source_entries,
    state_result_switch_logits,
    retention_bound_margin,
    extra_fading_amount,
    state_result_scale,
    state_result_matrix,
    second_slice_tokens,
    specialist_assignment,
    selected_specialist_share,
    leading_scale_vector,
    trailing_scale_vector,
    specialist_switch_matrix,
    specialist_widen_matrix,
    specialist_contract_matrix,
):
    _, width = state_probe_logits.shape
    members = lax.axis_size(EP)
    place = lax.axis_index("tp")
    ring = lax.axis_size("tp")
    features = second_slice_tokens.shape[1]

    own_route = lax.dynamic_slice_in_dim(specialist_assignment, place * TOK_DEV, TOK_DEV, 0)
    own_share = lax.dynamic_slice_in_dim(selected_specialist_share, place * TOK_DEV, TOK_DEV, 0)
    own_rows = lax.dynamic_slice_in_dim(second_slice_tokens, place * TOK_DEV, TOK_DEV, 0)

    down_halves = halves(specialist_contract_matrix[0], 0)
    down_halves, own_rows = lax.optimization_barrier((down_halves, own_rows))
    downs = widened(specialist_contract_matrix[0], down_halves)
    gates = widened(specialist_switch_matrix[0], halves(specialist_switch_matrix[0], 1))
    up_halves = halves(specialist_widen_matrix[0], 1)
    up_halves, retention_logits = lax.optimization_barrier((up_halves, retention_logits))
    ups = widened(specialist_widen_matrix[0], up_halves)
    normed = rms_scale(own_rows.astype(F32), leading_scale_vector).astype(BF16)
    experts = specialist_switch_matrix.shape[0] * members
    capacity = 2 * TOK_DEV * own_route.shape[1] // experts
    expert_ids = jnp.arange(experts, dtype=jnp.int32)[:, None]
    named = [(own_route[:, k][None, :] == expert_ids) for k in range(own_route.shape[1])]
    member = functools.reduce(jnp.logical_or, named)
    weight = sum(jnp.where(named[k], own_share[:, k][None, :], 0.0) for k in range(len(named)))
    ahead = jnp.arange(TOK_DEV)[:, None] < jnp.arange(TOK_DEV)[None, :]
    rank = jnp.dot(
        member.astype(BF16), ahead.astype(BF16), preferred_element_type=F32
    ).astype(jnp.int32)

    def slots_of(first, count):
        ids = first + jnp.arange(count, dtype=jnp.int32)
        return member[:, None, :] & (rank[:, None, :] == ids[None, :, None])

    pick = slots_of(0, capacity).astype(BF16).reshape(experts * capacity, TOK_DEV)
    packed = jnp.dot(pick, normed, preferred_element_type=F32).astype(BF16)
    arrived = exchange(packed.reshape(experts, capacity, features))

    raw, qdec, ends = local_pass(
        state_probe_logits,
        retention_logits,
        state_source_entries,
        retention_bound_margin,
        extra_fading_amount,
    )
    ends = ends.reshape(members, width // members, 2 * HEAD)
    ends, arrived = lax.optimization_barrier((ends, arrived))
    slices = exchange(ends)

    shares = []
    for k in range(GROUPS):
        chosen = slots_of(k * (capacity // GROUPS), capacity // GROUPS)
        share = jnp.where(chosen, weight[:, None, :], 0.0).reshape(-1, TOK_DEV)
        coarse = share.astype(BF16)
        fine = (share - coarse.astype(F32)).astype(BF16)
        shares.append((coarse, fine))

    combined = jnp.zeros((TOK_DEV, features), F32)
    count = capacity // GROUPS
    n = members * count // CHUNKS
    flat_in = arrived.reshape(CHUNKS, -1, features)
    at = jnp.arange(n, dtype=jnp.int32)
    where = at // count * capacity + at % count
    owns = []
    for k in range(GROUPS):
        chosen = (where + k * count)[:, None] == jnp.arange(flat_in.shape[1])[None, :]
        for c in range(CHUNKS):
            owns.append(
                jnp.dot(chosen.astype(BF16), flat_in[c], preferred_element_type=F32).astype(BF16)
            )
    parts = []
    for k in range(GROUPS):
        for c in range(CHUNKS):
            i = k * CHUNKS + c
            own = owns[i]
            far = shift(own, 2)
            parts.append(expert_block(own, far, gates, ups, downs))
            if i == 1:
                leaving = prefix_pass(slices)
    for k in range(GROUPS):
        finished = []
        for c in range(CHUNKS):
            mine, other = parts[k * CHUNKS + c]
            back = shift(other, 2)
            total = (mine.astype(F32) + back.astype(F32)).astype(BF16)
            if k == 0:
                beside = leaving.reshape(CHUNKS, n, HEAD)[c]
                total = jnp.concatenate([total, beside], axis=1)
            finished.append(total)
        finished = jnp.concatenate(finished, axis=0).reshape(members, count, -1)
        returned = exchange(finished)
        if k == 0:
            entering = returned[:, :, features:].reshape(width, HEAD)
            returned = returned[:, :, :features]
            rec = output_pass(raw, qdec, entering, state_result_switch_logits, state_result_scale)
        coarse, fine = shares[k]
        flat = returned.reshape(members * count, features)
        if k == GROUPS - 1:
            moe_out = finish(flat, coarse, fine, combined, trailing_scale_vector)
        else:
            for piece in (coarse, fine):
                combined = combined + lax.dot_general(
                    piece, flat, (((0,), (0,)), ((), ())), preferred_element_type=F32
                )

    own, far, left, right = rec, shift(rec, 2), shift(rec, 1), shift(rec, -1)
    by_block = state_result_matrix.reshape(ring, width, -1)

    def columns(block, at):
        held = lax.dynamic_index_in_dim(by_block, lax.rem(place + at, ring), 0, keepdims=False)
        return jnp.dot(block, held, preferred_element_type=F32)

    mixed = columns(own, 0) + columns(left, ring - 1) + columns(right, 1) + columns(far, 2)
    mixer_out = mixed.astype(BF16)
    return (mixer_out, moe_out)


def solution(mesh):
    finer = Mesh(mesh.devices.reshape(8, 4, 2, mesh.shape["tp"]), ("ep_0", "ep_1", "ep_2", "tp"))
    placed = (
        P(EP, "tp"),
        P(EP, "tp"),
        P(EP, "tp"),
        P(EP, "tp"),
        P("tp"),
        P(EP, "tp"),
        P("tp"),
        P(None, "tp"),
        P(EP, None),
        P(EP, None),
        P(EP, None),
        P(),
        P(),
        P(EP, None, "tp"),
        P(EP, None, "tp"),
        P(EP, "tp", None),
    )

    return jax.shard_map(
        shards,
        mesh=finer,
        in_specs=placed,
        out_specs=(P(EP, "tp"), P(EP_TP, None)),
        check_vma=False,
    )
```
